512 devices in a mesh: ep: 32 (over z, x), tp: 16 (over y, core).
Axes of the slice: x: 4, y: 8, z: 8, core: 2. Of those that a mesh axis runs over, the one named last changes fastest.
Arguments:
- pool_input: bfloat16 [8192, 2048], P('ep', 'tp'), may hold values from -6 to 6
- pool_map: bfloat16 [16, 128, 128], replicated, may hold values from -0.5 to 0.5
- pool_scale: float32 [2048], replicated, may hold values from 0.1 to 1.9
- out_proj: bfloat16 [2048, 4096], P('tp'), may hold values from -0.125 to 0.125
- moe_input: bfloat16 [4096, 4096], P('ep'), may hold values from -6 to 6
- norm_gain: float32 [4096], replicated, may hold values from 0.1 to 1.9
- routes: int32 [4096, 4], P('ep'), may hold values from 0 to 31, all different within a row; in each aligned block of 128 rows (0 to 127, 128 to 255, ...) at most 24 rows name the same one
- route_weights: float32 [4096, 4], P('ep'), may hold values from 0.1 to 1
- expert_gate: bfloat16 [32, 4096, 1024], P('ep', None, 'tp'), may hold values from -0.09375 to 0.09375
- expert_up: bfloat16 [32, 4096, 1024], P('ep', None, 'tp'), may hold values from -0.09375 to 0.09375
- expert_down: bfloat16 [32, 1024, 4096], P('ep', None, 'tp'), may hold values from -0.1875 to 0.1875
- shared_gate: bfloat16 [4096, 512], P(None, 'tp'), may hold values from -0.09375 to 0.09375
- shared_up: bfloat16 [4096, 512], P(None, 'tp'), may hold values from -0.09375 to 0.09375
- shared_down: bfloat16 [512, 4096], P('tp'), may hold values from -0.25 to 0.25
Outputs:
- mixer_output: bfloat16 [8192, 4096], P('ep', 'tp')
- moe_output: bfloat16 [4096, 4096], P('ep', 'tp')
The draws below stay inside these ranges and needn't reach their ends.
Inputs may be any that keep to these rules, and one draw needn't show every extreme that they name: `routes`: each row names 4 different experts. In each aligned block of 128 rows no expert is named by more than 24 rows, a bound that some block reaches.
All inputs are finite; a program needn't handle non-finite values.
Results may differ from the reference program's by a relative error of at most 0.017.
Values may be sent and summed in bfloat16 or wider, within the bound.
No kernel may reach another device: no remote copies, remote signals or barrier semaphores. Data moves between devices by JAX's collectives and lax.ppermute only.
A program may use at most 64 MiB of HBM per device.

```python
import math
import jax
import jax.numpy as jnp
import numpy as np
from jax import lax

D = 4096
POOL_WIDTH = 2048
POOL_GROUPS = 16
GROUP_DIM = 128
EXPERT_DIM = 1024
SHARED_DIM = 512
TOP_K = 4
TOK2_DEV = 128
TOK1 = 8192
TOK2 = 4096
EXPERTS = 32
CAP = 24
EXPERT_ROWS = 768
N_EP = 32
N_TP = 16


def level_of(key, extent, pieces, smallest, largest):
    gain, own = 1.0, jax.random.fold_in(key, 6)
    for dim, blocks in pieces:
        steps = jnp.exp(jax.random.uniform(jax.random.fold_in(own, dim), (blocks,), jnp.float32, smallest / len(pieces), largest / len(pieces)))
        gain = gain * jnp.repeat(steps, extent[dim] // blocks).reshape([-1 if axis == dim else 1 for axis in range(len(extent))])
    return gain


def routed_block(own_key, own, number, rows, number_of, top, reach, lean):
    ranking = jax.random.permutation(own_key, number_of)
    heavy_load, common = load_shares(number_of, rows * top, reach, lean, True), load_shares(number_of, rows * top, reach, lean, False)
    places = jnp.arange(number_of)

    def named(lengths, offset_by):
        used = int((lengths > 0).sum())
        fixed = max(1, used // 4)
        shifted = fixed + (places - fixed + offset_by * (used - fixed)) % max(1, number_of - fixed)
        return jnp.zeros((number_of,), jnp.int32).at[ranking[jnp.where(places < fixed, places, shifted)]].set(jnp.asarray(lengths, jnp.int32))

    lengths = jnp.where(number % 4 == 0, named(heavy_load, number // 4), named(common, number - number // 4 - 1))
    mixed = jax.random.permutation(jax.random.fold_in(own, 3), number_of)
    giver, receiver = mixed[0:number_of // 2 * 2:2], mixed[1:number_of // 2 * 2:2]
    margin = jnp.minimum(lengths[giver] - 1, reach - lengths[receiver]) // 2
    margin = jnp.where((giver == ranking[0]) | (receiver == ranking[0]) | (lengths[receiver] == 0), 0, jnp.maximum(margin, 0))
    shifted = jax.random.randint(jax.random.fold_in(own, 4), (number_of // 2,), 0, 1 << 20) % (margin + 1)
    lengths = lengths.at[giver].add(-shifted).at[receiver].add(shifted)
    members = jnp.searchsorted(jnp.cumsum(lengths), jnp.arange(rows * top), side="right").astype(jnp.int32)
    grid = members.reshape(top, rows).T
    grid = grid[jax.random.permutation(jax.random.fold_in(own, 1), rows)]
    offset_by = jax.random.randint(jax.random.fold_in(own, 2), (rows, 1), 0, top)
    return jnp.take_along_axis(grid, (jnp.arange(top)[None, :] + offset_by) % top, axis=1)


def load_shares(amount, total, limit, slope, full):
    loads = [(1 << 20) // math.isqrt(rank ** slope) + 1 for rank in range(1, amount + 1)]
    largest = limit if full else min(limit, max(-(-total // amount), total * loads[0] // sum(loads)))
    least = 1 if total - largest >= amount - 1 else 0
    given, spare = [largest] + [least] * (amount - 1), total - largest - least * (amount - 1)
    while spare > 0:
        candidates = [i for i in range(1, amount) if given[i] < largest] or [i for i in range(1, amount) if given[i] < limit]
        whole, left = sum([loads[i] for i in candidates]), spare
        for i in candidates:
            addition = min(limit - given[i], max(1, left * loads[i] // whole), spare)
            given[i] = given[i] + addition
            spare = spare - addition
    return np.array(given)


def bell_draw(key, shape, spread, reach, shards=(), kind=jnp.bfloat16):
    entries = jax.random.normal(key, shape, jnp.float32) * spread
    if len(shards) > 0:
        entries = level_of(key, shape, shards, -0.22, 0.18) * entries
    return jnp.clip(entries, min=-reach, max=reach).astype(kind)


def setup_inputs(seed: int = 0) -> dict:
    arg_keys = jax.random.split(jax.random.key(seed), 15)
    pool_input = bell_draw(arg_keys[0], (TOK1, POOL_WIDTH), 1.0, 6.0, ((0, 32), (1, 16)))
    pool_map = bell_draw(arg_keys[1], (POOL_GROUPS, GROUP_DIM, GROUP_DIM), GROUP_DIM ** -0.5, 0.5)
    pool_scale = jnp.clip(1.0 + 0.18 * jax.random.normal(arg_keys[2], (POOL_WIDTH,), jnp.float32), 0.1, 1.9)
    out_proj = bell_draw(arg_keys[3], (POOL_WIDTH, D), POOL_WIDTH ** -0.5, 0.125, ((0, 16),))
    moe_input = bell_draw(arg_keys[4], (TOK2, D), 1.0, 6.0, ((0, 32),))
    norm_gain = jnp.clip(1.0 + 0.18 * jax.random.normal(arg_keys[5], (D,), jnp.float32), 0.1, 1.9)
    routes_keys = jax.random.split(jax.random.fold_in(arg_keys[6], 1), TOK2 // TOK2_DEV)
    routes_turns = jax.random.permutation(jax.random.fold_in(arg_keys[6], 3), TOK2 // TOK2_DEV)
    routes = jax.vmap(lambda own, number: routed_block(jax.random.fold_in(arg_keys[6], 2), own, number, TOK2_DEV, EXPERTS, TOP_K, CAP, 1))(routes_keys, routes_turns).reshape((TOK2, TOP_K))
    route_weights = jnp.clip(jnp.exp(math.log(1.0) - 2.3025851 * jax.random.uniform(arg_keys[7], (TOK2, TOP_K), jnp.float32) ** level_of(arg_keys[7], (TOK2, TOP_K), ((0, 32),), -0.2, 0.2)), 0.1, 1.0)
    expert_gate = bell_draw(arg_keys[8], (EXPERTS, D, EXPERT_DIM), D ** -0.5, 0.09375, ((0, 32), (2, 16)))
    expert_up = bell_draw(arg_keys[9], (EXPERTS, D, EXPERT_DIM), D ** -0.5, 0.09375, ((0, 32), (2, 16)))
    expert_down = bell_draw(arg_keys[10], (EXPERTS, EXPERT_DIM, D), EXPERT_DIM ** -0.5, 0.1875, ((0, 32), (2, 16)))
    shared_gate = bell_draw(arg_keys[11], (D, SHARED_DIM), D ** -0.5, 0.09375, ((1, 16),))
    shared_up = bell_draw(arg_keys[12], (D, SHARED_DIM), D ** -0.5, 0.09375, ((1, 16),))
    shared_down = bell_draw(arg_keys[13], (SHARED_DIM, D), SHARED_DIM ** -0.5, 0.25, ((0, 16),))
    return {"pool_input": pool_input, "pool_map": pool_map, "pool_scale": pool_scale, "out_proj": out_proj, "moe_input": moe_input, "norm_gain": norm_gain, "routes": routes, "route_weights": route_weights, "expert_gate": expert_gate, "expert_up": expert_up, "expert_down": expert_down, "shared_gate": shared_gate, "shared_up": shared_up, "shared_down": shared_down}


windows = (2, 4, 8, 16)
reach_back = 15
eps = 1e-05

def pool_mixer(pool_input, pool_map, pool_scale, out_proj):
    row_count = pool_input.shape[0]
    channels = pool_input.shape[1]
    values = pool_input.astype(jnp.float32)
    padded = jnp.concatenate([jnp.zeros((reach_back, channels), jnp.float32), values], axis=0)
    position = jnp.arange(row_count, dtype=jnp.float32)
    group_kind = jnp.arange(channels, dtype=jnp.int32) // GROUP_DIM % 4
    running = jnp.zeros((row_count, channels), jnp.float32)
    pooled = -values
    for lag_step in range(reach_back + 1):
        running = running + padded[reach_back - lag_step:reach_back - lag_step + row_count]
        if lag_step + 1 in windows:
            kind_id = windows.index(lag_step + 1)
            counts = jnp.minimum(position + 1.0, float(lag_step + 1))
            select = (group_kind == kind_id).astype(jnp.float32)
            pooled = pooled + select[None, :] * running / counts[:, None]
    pooled = pooled.astype(jnp.bfloat16)
    grouped = pooled.reshape(row_count, POOL_GROUPS, GROUP_DIM).astype(jnp.float32)
    mapped = jnp.einsum('rgc,gcd->rgd', grouped, pool_map.astype(jnp.float32)).reshape(row_count, channels)
    group_out = (mapped * pool_scale[None, :]).astype(jnp.bfloat16)
    block_width = channels // N_TP
    mixed = jnp.zeros((row_count, out_proj.shape[1]), jnp.float32)
    for block_idx in range(N_TP):
        lower = block_idx * block_width
        partial_sum = jnp.dot(group_out[:, lower:lower + block_width], out_proj[lower:lower + block_width], preferred_element_type=jnp.float32).astype(jnp.bfloat16)
        partial_sum = lax.optimization_barrier(partial_sum)
        mixed = mixed + partial_sum.astype(jnp.float32)
    return mixed.astype(jnp.bfloat16)

def slot_rows(routes):
    blocks = routes.reshape(N_EP, TOK2_DEV * TOP_K)
    one_hot = (blocks[:, :, None] == jnp.arange(EXPERTS, dtype=jnp.int32)[None, None, :]).astype(jnp.int32)
    earlier = jnp.cumsum(one_hot, axis=1) - one_hot
    slot_ids = lax.optimization_barrier(jnp.sum(earlier * one_hot, axis=2))
    block_ids = jnp.arange(N_EP, dtype=jnp.int32)[:, None]
    buffer_row = blocks * EXPERT_ROWS + block_ids * CAP + slot_ids
    return buffer_row.reshape(TOK2, TOP_K).astype(jnp.int32)

def one_expert(operands):
    rows_in, gate_weight, up_weight, down_weight = operands
    gate_val = jnp.dot(rows_in, gate_weight, preferred_element_type=jnp.float32)
    up_val = jnp.dot(rows_in, up_weight, preferred_element_type=jnp.float32)
    hidden = (jax.nn.silu(gate_val) * up_val).astype(jnp.bfloat16)
    return jnp.dot(hidden, down_weight, preferred_element_type=jnp.float32).astype(jnp.bfloat16)

def moe_layer(moe_input, norm_gain, routes, route_weights, expert_gate, expert_up, expert_down, shared_gate, shared_up, shared_down):
    values = moe_input.astype(jnp.float32)
    centre = values - lax.optimization_barrier(jnp.mean(values, axis=1, keepdims=True))
    variance = lax.optimization_barrier(jnp.mean(centre * centre, axis=1, keepdims=True))
    normed = (centre * lax.rsqrt(variance + eps) * norm_gain[None, :]).astype(jnp.bfloat16)
    buffer_row = slot_rows(routes)
    repeated = jnp.repeat(normed, TOP_K, axis=0)
    buffers = jnp.zeros((EXPERTS * EXPERT_ROWS, D), jnp.bfloat16).at[buffer_row.reshape(-1)].set(repeated)
    buffers = buffers.reshape(EXPERTS, EXPERT_ROWS, D)
    expert_out = lax.map(one_expert, (buffers, expert_gate, expert_up, expert_down))
    expert_out = expert_out.reshape(EXPERTS * EXPERT_ROWS, D)
    routed = jnp.zeros((TOK2, D), jnp.float32)
    for top_step in range(TOP_K):
        picked = expert_out[buffer_row[:, top_step]].astype(jnp.float32)
        routed = routed + route_weights[:, top_step, None] * picked
    shared_gate_val = jnp.dot(normed, shared_gate, preferred_element_type=jnp.float32)
    shared_up_val = jnp.dot(normed, shared_up, preferred_element_type=jnp.float32)
    shared_hidden = (jax.nn.silu(shared_gate_val) * shared_up_val).astype(jnp.bfloat16)
    block_width = SHARED_DIM // N_TP
    shared_sum = jnp.zeros((TOK2, D), jnp.float32)
    for block_idx in range(N_TP):
        lower = block_idx * block_width
        partial_sum = jnp.dot(shared_hidden[:, lower:lower + block_width], shared_down[lower:lower + block_width], preferred_element_type=jnp.float32).astype(jnp.bfloat16)
        partial_sum = lax.optimization_barrier(partial_sum)
        shared_sum = shared_sum + partial_sum.astype(jnp.float32)
    return (routed + shared_sum).astype(jnp.bfloat16)

def reference(pool_input, pool_map, pool_scale, out_proj, moe_input, norm_gain, routes, route_weights, expert_gate, expert_up, expert_down, shared_gate, shared_up, shared_down):
    mixer_output = pool_mixer(pool_input, pool_map, pool_scale, out_proj)
    moe_output = moe_layer(moe_input, norm_gain, routes, route_weights, expert_gate, expert_up, expert_down, shared_gate, shared_up, shared_down)
    return (mixer_output, moe_output)
```

```python
import jax
import jax.numpy as jnp
from jax import lax
from jax.sharding import PartitionSpec as P

windows = (2, 4, 8, 16)
reach_back = 15
eps = 1e-05
f32 = jnp.float32
bf16 = jnp.bfloat16


def halo(block):
    devices = range(lax.axis_size("ep"))
    return lax.ppermute(block, "ep", [(i - 1, i) for i in devices if i > 0])


def along_y(x, step):
    n = lax.axis_size("tp")
    return lax.ppermute(x, "tp", [(i, (i + 2 * step) % n) for i in range(n)])


def to_partner(x):
    n = lax.axis_size("tp")
    return lax.ppermute(x, "tp", [(i, i ^ 1) for i in range(n)])


def tdot(a, b):
    return lax.dot_general(a, b, (((1,), (1,)), ((), ())), preferred_element_type=f32)


def pool_group_out(pool_input, earlier_rows, pool_map, pool_scale, tp_rank, ep_rank):
    row_count, channels = pool_input.shape
    group_dim = pool_map.shape[1]
    local_groups = channels // group_dim
    values = pool_input.astype(f32)
    extended = jnp.concatenate([earlier_rows.astype(f32), values], axis=0)
    position = (ep_rank * row_count + jnp.arange(row_count, dtype=jnp.int32)).astype(f32)
    group_ids = tp_rank * local_groups + jnp.arange(channels, dtype=jnp.int32) // group_dim
    group_kind = group_ids % 4
    running = jnp.zeros((row_count, channels), f32)
    pooled = -values
    for lag_step in range(reach_back + 1):
        running = running + extended[reach_back - lag_step : reach_back - lag_step + row_count]
        if lag_step + 1 in windows:
            kind_id = windows.index(lag_step + 1)
            counts = jnp.minimum(position + 1.0, float(lag_step + 1))
            select = (group_kind == kind_id).astype(f32)
            pooled = pooled + select[None, :] * running / counts[:, None]
    pooled = pooled.astype(bf16)
    my_maps = lax.dynamic_slice_in_dim(pool_map, tp_rank * local_groups, local_groups, 0)
    my_scale = lax.dynamic_slice_in_dim(pool_scale, tp_rank * channels, channels, 0)
    mapped = jnp.einsum(
        "rgc,gcd->rgd",
        pooled.reshape(row_count, local_groups, group_dim),
        my_maps,
        preferred_element_type=f32,
    )
    return (mapped.reshape(row_count, channels) * my_scale[None, :]).astype(bf16)


def per_device(
    pool_input,
    pool_map,
    pool_scale,
    out_proj,
    moe_input,
    norm_gain,
    routes,
    route_weights,
    expert_gate,
    expert_up,
    expert_down,
    shared_gate,
    shared_up,
    shared_down,
):
    tp_rank = lax.axis_index("tp")
    ep_rank = lax.axis_index("ep")
    tp_size = lax.axis_size("tp")
    expert_count = lax.axis_size("ep")
    y_size = tp_size // 2
    core = tp_rank % 2
    y = tp_rank // 2
    tok_count, width = moe_input.shape
    top_count = routes.shape[1]
    capacity = (3 * tok_count * top_count + 2 * expert_count - 1) // (2 * expert_count)
    buffer_len = expert_count * capacity
    slice_width = width // tp_size
    row_count = pool_input.shape[0]

    earlier_rows = halo(pool_input[row_count - reach_back :])

    routes_t = routes.T
    experts = jnp.arange(expert_count, dtype=jnp.int32)[:, None]
    named = jnp.zeros((expert_count, tok_count), f32)
    weight_t = jnp.zeros((expert_count, tok_count), f32)
    for k in range(top_count):
        hit = routes_t[k][None, :] == experts
        named = named + hit.astype(f32)
        weight_t = weight_t + jnp.where(hit, route_weights.T[k][None, :], 0.0)
    before = jnp.arange(tok_count)[:, None] < jnp.arange(tok_count)[None, :]
    earlier = jnp.dot(named.astype(bf16), before.astype(bf16), preferred_element_type=f32)
    slot = jnp.where(named > 0, earlier, -1.0)
    slots = jnp.arange(capacity, dtype=f32)[None, :, None]
    match = slot[:, None, :] == slots
    placing = match.astype(bf16).reshape(buffer_len, tok_count)
    combine = jnp.where(match, weight_t[:, None, :], 0.0).astype(bf16).reshape(buffer_len, tok_count)

    values = moe_input.astype(f32)
    mean = jnp.mean(values, axis=1, keepdims=True)
    centre = values - mean
    rstd = lax.rsqrt(jnp.mean(centre * centre, axis=1, keepdims=True) + eps)
    at = tp_rank * slice_width
    mine = lax.dynamic_slice_in_dim(moe_input, at, slice_width, 1).astype(f32)
    my_gain = lax.dynamic_slice_in_dim(norm_gain, at, slice_width, 0)
    normed_slice = ((mine - mean) * rstd * my_gain[None, :]).astype(bf16)
    outgoing = jnp.dot(placing, normed_slice, preferred_element_type=f32).astype(bf16)
    arrived = lax.all_to_all(outgoing, "ep", split_axis=0, concat_axis=0, tiled=True)

    gate_up = jnp.concatenate([expert_gate[0].T, expert_up[0].T], axis=0)
    hid = gate_up.shape[0]

    def feature_slices(side):
        pieces = []
        for j in range(y_size):
            lo = 2 * j * slice_width
            even = gate_up[:, lo : lo + slice_width]
            odd = gate_up[:, lo + slice_width : lo + 2 * slice_width]
            pieces.append(jnp.where(side == 0, even, odd))
        return jnp.stack(pieces)

    own_weights = feature_slices(core)
    partner_weights = to_partner(feature_slices(1 - core))
    weights = jnp.concatenate([own_weights, partner_weights], axis=1)

    def product(rows, offset):
        w = lax.dynamic_index_in_dim(weights, (y + offset) % y_size, 0, keepdims=False)
        return tdot(w, rows)

    half = buffer_len // 2
    sums = []
    ups = [rows for rows in (arrived[:half], arrived[half:])]
    downs = list(ups)
    sums = [product(rows, 0) for rows in ups]
    reach_up = (y_size // 2, y_size // 2 - 1)
    for step in range(1, y_size // 2 + 1):
        for h in range(2):
            if step <= reach_up[h]:
                ups[h] = along_y(ups[h], 1)
                sums[h] = sums[h] + product(ups[h], -step)
            if step <= reach_up[1 - h]:
                downs[h] = along_y(downs[h], -1)
                sums[h] = sums[h] + product(downs[h], step)
    partial = jnp.concatenate(sums, axis=1)
    full = partial[:hid] + to_partner(partial[hid:])
    units = hid // 2
    hidden = (jax.nn.silu(full[:units]) * full[units:]).astype(bf16)

    order = [None] * y_size
    order[0] = hidden
    up = down = hidden
    for step in range(1, y_size // 2 + 1):
        up = along_y(up, 1)
        order[y_size - step] = up
        if step < y_size // 2:
            down = along_y(down, -1)
            order[step] = down
    own_hidden = jnp.concatenate(order, axis=0)
    other_hidden = to_partner(own_hidden)
    down_weight = expert_down[0].reshape(y_size, 2, units, slice_width)

    def down_rows(side):
        pieces = []
        for j in range(y_size):
            block = lax.dynamic_index_in_dim(down_weight, (y + j) % y_size, 0, keepdims=False)
            pieces.append(jnp.where(side == 0, block[0], block[1]))
        return jnp.concatenate(pieces, axis=0)

    def down_product(h, w):
        return lax.dot_general(h, w, (((0,), (0,)), ((), ())), preferred_element_type=f32)

    expert_result = down_product(own_hidden, down_rows(core))
    expert_result = expert_result + down_product(other_hidden, down_rows(1 - core))
    returned = lax.all_to_all(expert_result.astype(bf16), "ep", split_axis=0, concat_axis=0, tiled=True)
    routed = lax.dot_general(combine, returned, (((0,), (0,)), ((), ())), preferred_element_type=f32)

    group_out = pool_group_out(pool_input, earlier_rows, pool_map, pool_scale, tp_rank, ep_rank)
    normed = (centre * rstd * norm_gain[None, :]).astype(bf16)
    shared_gate_val = jnp.dot(normed, shared_gate, preferred_element_type=f32)
    shared_up_val = jnp.dot(normed, shared_up, preferred_element_type=f32)
    shared_hidden = (jax.nn.silu(shared_gate_val) * shared_up_val).astype(bf16)

    def columns(weight, side):
        pieces = []
        for j in range(y_size):
            begin = (((y + j) % y_size) * 2 + side) * slice_width
            pieces.append(lax.dynamic_slice_in_dim(weight, begin, slice_width, 1))
        return jnp.concatenate(pieces, axis=1)

    def projected(side):
        top = jnp.dot(group_out, columns(out_proj, side), preferred_element_type=f32)
        bottom = jnp.dot(shared_hidden, columns(shared_down, side), preferred_element_type=f32)
        return jnp.concatenate([top.astype(bf16), bottom.astype(bf16)], axis=0)

    from_partner = to_partner(projected(1 - core))
    kept = projected(core)

    def part(j):
        lo = j * slice_width
        return kept[:, lo : lo + slice_width].astype(f32) + from_partner[:, lo : lo + slice_width].astype(f32)

    up = down = None
    for step in range(y_size // 2):
        j = y_size // 2 - step
        up = part(j) if up is None else part(j) + up.astype(f32)
        up = along_y(up.astype(bf16), 1)
        if step < y_size // 2 - 1:
            j = y_size // 2 + 1 + step
            down = part(j) if down is None else part(j) + down.astype(f32)
            down = along_y(down.astype(bf16), -1)
    total = part(0) + up.astype(f32) + down.astype(f32)
    return (total[:row_count].astype(bf16), (routed + total[row_count:]).astype(bf16))


def solution(mesh):
    return jax.shard_map(
        per_device,
        mesh=mesh,
        in_specs=(
            P("ep", "tp"),
            P(),
            P(),
            P("tp", None),
            P("ep", None),
            P(),
            P("ep", None),
            P("ep", None),
            P("ep", None, "tp"),
            P("ep", None, "tp"),
            P("ep", None, "tp"),
            P(None, "tp"),
            P(None, "tp"),
            P("tp", None),
        ),
        out_specs=(P("ep", "tp"), P("ep", "tp")),
        check_vma=False,
    )
```

```python
import jax
import jax.numpy as jnp
from jax import lax
from jax.experimental import pallas as pl
from jax.experimental.pallas import tpu as pltpu
from jax.sharding import PartitionSpec as P

windows = (2, 4, 8, 16)
reach_back = 15
eps = 1e-05
f32 = jnp.float32
bf16 = jnp.bfloat16


def halo(block):
    devices = range(lax.axis_size("ep"))
    return lax.ppermute(block, "ep", [(i - 1, i) for i in devices if i > 0])


def along_y(x, step):
    n = lax.axis_size("tp")
    return lax.ppermute(x, "tp", [(i, (i + 2 * step) % n) for i in range(n)])


def to_partner(x):
    n = lax.axis_size("tp")
    return lax.ppermute(x, "tp", [(i, i ^ 1) for i in range(n)])


def tdot(a, b):
    return lax.dot_general(a, b, (((1,), (1,)), ((), ())), preferred_element_type=f32)


def gate_up_kernel(index, gate_own, up_own, gate_out, up_out, own, out):
    units = gate_own.shape[0]
    own[0, :units] = gate_own[...]
    own[0, units:] = up_own[...]
    out[0, :units] = gate_out[...]
    out[0, units:] = up_out[...]


def gate_up_blocks(index, gate_t, up_t, slice_width):
    units = gate_t.shape[0]
    count = index.shape[1]
    block = (units, slice_width)
    own = pl.BlockSpec(block, lambda j, index: (0, index[0, j]))
    out = pl.BlockSpec(block, lambda j, index: (0, index[1, j]))
    result = pl.BlockSpec((1, 2 * units, slice_width), lambda j, index: (j, 0, 0))
    shape = jax.ShapeDtypeStruct((count, 2 * units, slice_width), bf16)
    return pl.pallas_call(
        gate_up_kernel,
        grid_spec=pltpu.PrefetchScalarGridSpec(
            num_scalar_prefetch=1, grid=(count,), in_specs=[own, own, out, out], out_specs=[result, result]
        ),
        out_shape=[shape, shape],
    )(index, gate_t, up_t, gate_t, up_t)


def project_kernel(index, group, hidden, proj_own, proj_out, down_own, down_out, own, out):
    rows = group.shape[0]
    for proj, down, to in ((proj_own, down_own, own), (proj_out, down_out, out)):
        to[0, :rows] = jnp.dot(group[...], proj[...], preferred_element_type=f32).astype(bf16)
        to[0, rows:] = jnp.dot(hidden[...], down[...], preferred_element_type=f32).astype(bf16)


def projected_blocks(index, group_out, shared_hidden, out_proj, shared_down, slice_width):
    count = index.shape[1]
    rows = group_out.shape[0] + shared_hidden.shape[0]

    def whole(a):
        return pl.BlockSpec(a.shape, lambda j, index: (0, 0))

    def columns(a, side):
        return pl.BlockSpec((a.shape[0], slice_width), lambda j, index: (0, index[side, j]))

    result = pl.BlockSpec((1, rows, slice_width), lambda j, index: (j, 0, 0))
    shape = jax.ShapeDtypeStruct((count, rows, slice_width), bf16)
    return pl.pallas_call(
        project_kernel,
        grid_spec=pltpu.PrefetchScalarGridSpec(
            num_scalar_prefetch=1,
            grid=(count,),
            in_specs=[
                whole(group_out),
                whole(shared_hidden),
                columns(out_proj, 0),
                columns(out_proj, 1),
                columns(shared_down, 0),
                columns(shared_down, 1),
            ],
            out_specs=[result, result],
        ),
        out_shape=[shape, shape],
    )(index, group_out, shared_hidden, out_proj, out_proj, shared_down, shared_down)


def pool_group_out(pool_input, earlier_rows, pool_map, pool_scale, tp_rank, ep_rank):
    row_count, channels = pool_input.shape
    group_dim = pool_map.shape[1]
    local_groups = channels // group_dim
    values = pool_input.astype(f32)
    extended = jnp.concatenate([earlier_rows.astype(f32), values], axis=0)
    position = (ep_rank * row_count + jnp.arange(row_count, dtype=jnp.int32)).astype(f32)
    group_ids = tp_rank * local_groups + jnp.arange(channels, dtype=jnp.int32) // group_dim
    group_kind = group_ids % 4
    running = jnp.zeros((row_count, channels), f32)
    pooled = -values
    for lag_step in range(reach_back + 1):
        running = running + extended[reach_back - lag_step : reach_back - lag_step + row_count]
        if lag_step + 1 in windows:
            kind_id = windows.index(lag_step + 1)
            counts = jnp.minimum(position + 1.0, float(lag_step + 1))
            select = (group_kind == kind_id).astype(f32)
            pooled = pooled + select[None, :] * running / counts[:, None]
    pooled = pooled.astype(bf16)
    my_maps = lax.dynamic_slice_in_dim(pool_map, tp_rank * local_groups, local_groups, 0)
    my_scale = lax.dynamic_slice_in_dim(pool_scale, tp_rank * channels, channels, 0)
    mapped = jnp.einsum(
        "rgc,gcd->rgd",
        pooled.reshape(row_count, local_groups, group_dim),
        my_maps,
        preferred_element_type=f32,
    )
    return (mapped.reshape(row_count, channels) * my_scale[None, :]).astype(bf16)


def per_device(
    pool_input,
    pool_map,
    pool_scale,
    out_proj,
    moe_input,
    norm_gain,
    routes,
    route_weights,
    expert_gate,
    expert_up,
    expert_down,
    shared_gate,
    shared_up,
    shared_down,
):
    tp_rank = lax.axis_index("tp")
    ep_rank = lax.axis_index("ep")
    tp_size = lax.axis_size("tp")
    expert_count = lax.axis_size("ep")
    y_size = tp_size // 2
    core = tp_rank % 2
    y = tp_rank // 2
    tok_count, width = moe_input.shape
    top_count = routes.shape[1]
    capacity = (3 * tok_count * top_count + 2 * expert_count - 1) // (2 * expert_count)
    buffer_len = expert_count * capacity
    slice_width = width // tp_size
    row_count = pool_input.shape[0]

    earlier_rows = halo(pool_input[row_count - reach_back :])

    routes_t = routes.T
    experts = jnp.arange(expert_count, dtype=jnp.int32)[:, None]
    named = jnp.zeros((expert_count, tok_count), f32)
    weight_t = jnp.zeros((expert_count, tok_count), f32)
    for k in range(top_count):
        hit = routes_t[k][None, :] == experts
        named = named + hit.astype(f32)
        weight_t = weight_t + jnp.where(hit, route_weights.T[k][None, :], 0.0)
    before = jnp.arange(tok_count)[:, None] < jnp.arange(tok_count)[None, :]
    earlier = jnp.dot(named.astype(bf16), before.astype(bf16), preferred_element_type=f32)
    slot = jnp.where(named > 0, earlier, -1.0)
    slots = jnp.arange(capacity, dtype=f32)[None, :, None]
    match = slot[:, None, :] == slots
    placing = match.astype(bf16).reshape(buffer_len, tok_count)
    combine = jnp.where(match, weight_t[:, None, :], 0.0).astype(bf16).reshape(buffer_len, tok_count)

    values = moe_input.astype(f32)
    mean = jnp.mean(values, axis=1, keepdims=True)
    centre = values - mean
    rstd = lax.rsqrt(jnp.mean(centre * centre, axis=1, keepdims=True) + eps)

    def outgoing(far):
        at = (((y + far) % y_size) * 2 + core) * slice_width
        mine = lax.dynamic_slice_in_dim(moe_input, at, slice_width, 1).astype(f32)
        gain = lax.dynamic_slice_in_dim(norm_gain, at, slice_width, 0)
        normed_slice = ((mine - mean) * rstd * gain[None, :]).astype(bf16)
        return jnp.dot(placing, normed_slice, preferred_element_type=f32).astype(bf16)

    def exchanged(rows):
        return lax.all_to_all(rows, "ep", split_axis=0, concat_axis=0, tiled=True)

    near = exchanged(outgoing(0))
    far = exchanged(outgoing(y_size // 2))

    turn = (y + jnp.arange(y_size, dtype=jnp.int32)) % y_size
    index = jnp.stack([turn * 2 + core, turn * 2 + 1 - core]).astype(jnp.int32)
    own_weights, to_send = gate_up_blocks(index, expert_gate[0].T, expert_up[0].T, slice_width)
    partner_weights = to_partner(to_send)
    units = expert_gate.shape[2]

    sums = [0.0, 0.0]

    def add_product(rows, j):
        sums[0] = sums[0] + tdot(own_weights[j % y_size], rows)
        sums[1] = sums[1] + tdot(partner_weights[j % y_size], rows)

    up = along_y(near, 1)
    down = along_y(near, -1)
    add_product(near, 0)
    up_two = along_y(up, 1)
    down_two = along_y(down, -1)
    add_product(up, -1)
    add_product(down, 1)
    up_far = along_y(far, 1)
    down_far = along_y(far, -1)
    add_product(far, 4)
    add_product(up_two, -2)
    add_product(down_two, 2)
    add_product(up_far, 3)
    add_product(down_far, -3)
    full = sums[0] + to_partner(sums[1])
    hidden = (jax.nn.silu(full[:units]) * full[units:]).astype(bf16)

    copies = jnp.broadcast_to(hidden[None], (y_size, *hidden.shape))
    groups = [[2 * i + c for i in range(y_size)] for c in range(2)]
    own_hidden = lax.all_to_all(copies, "tp", 0, 0, axis_index_groups=groups, tiled=True)
    other_hidden = to_partner(own_hidden)
    down_weight = expert_down[0].reshape(y_size, 2, units, slice_width)

    def down_product(h, side):
        w = lax.dynamic_index_in_dim(down_weight, side, 1, keepdims=False)
        w = w.reshape(y_size * units, slice_width)
        return lax.dot_general(
            h.reshape(y_size * units, buffer_len), w, (((0,), (0,)), ((), ())), preferred_element_type=f32
        )

    expert_result = down_product(own_hidden, core) + down_product(other_hidden, 1 - core)
    returned = exchanged(expert_result.astype(bf16))
    routed = lax.dot_general(combine, returned, (((0,), (0,)), ((), ())), preferred_element_type=f32)

    group_out = pool_group_out(pool_input, earlier_rows, pool_map, pool_scale, tp_rank, ep_rank)
    normed = (centre * rstd * norm_gain[None, :]).astype(bf16)
    shared_gate_val = jnp.dot(normed, shared_gate, preferred_element_type=f32)
    shared_up_val = jnp.dot(normed, shared_up, preferred_element_type=f32)
    shared_hidden = (jax.nn.silu(shared_gate_val) * shared_up_val).astype(bf16)

    kept, sent = projected_blocks(index, group_out, shared_hidden, out_proj, shared_down, slice_width)
    from_partner = to_partner(sent)

    def part(j):
        return kept[j].astype(f32) + from_partner[j].astype(f32)

    up = down = None
    for step in range(y_size // 2):
        j = y_size // 2 - step
        up = part(j) if up is None else part(j) + up.astype(f32)
        up = along_y(up.astype(bf16), 1)
        if step < y_size // 2 - 1:
            j = y_size // 2 + 1 + step
            down = part(j) if down is None else part(j) + down.astype(f32)
            down = along_y(down.astype(bf16), -1)
    total = part(0) + up.astype(f32) + down.astype(f32)
    return (total[:row_count].astype(bf16), (routed + total[row_count:]).astype(bf16))


def solution(mesh):
    return jax.shard_map(
        per_device,
        mesh=mesh,
        in_specs=(
            P("ep", "tp"),
            P(),
            P(),
            P("tp", None),
            P("ep", None),
            P(),
            P("ep", None),
            P("ep", None),
            P("ep", None, "tp"),
            P("ep", None, "tp"),
            P("ep", None, "tp"),
            P(None, "tp"),
            P(None, "tp"),
            P("tp", None),
        ),
        out_specs=(P("ep", "tp"), P("ep", "tp")),
        check_vma=False,
    )
```

```python
import jax
import jax.numpy as jnp
from jax import lax
from jax.experimental import pallas as pl
from jax.experimental.pallas import tpu as pltpu
from jax.sharding import PartitionSpec as P


windows = (2, 4, 8, 16)
reach_back = 15
eps = 1e-05
f32 = jnp.float32
bf16 = jnp.bfloat16


def halo(block):
    devices = range(lax.axis_size("ep"))
    return lax.ppermute(block, "ep", [(i - 1, i) for i in devices if i > 0])


def along_y(x, step):
    n = lax.axis_size("tp")
    return lax.ppermute(x, "tp", [(i, (i + 2 * step) % n) for i in range(n)])


def to_partner(x):
    n = lax.axis_size("tp")
    return lax.ppermute(x, "tp", [(i, i ^ 1) for i in range(n)])


def tdot(a, b):
    return lax.dot_general(a, b, (((1,), (1,)), ((), ())), preferred_element_type=f32)


def lanes(block, width):
    return pl.ds(pl.multiple_of(block * width, width), width)


def local_kernel(body, index, operands, out_shape):
    vmem = pl.BlockSpec(memory_space=pltpu.VMEM)
    smem = pl.BlockSpec(memory_space=pltpu.SMEM)
    several = isinstance(out_shape, list)
    return pl.pallas_call(
        body,
        in_specs=[smem] + [vmem] * len(operands),
        out_specs=[vmem] * len(out_shape) if several else vmem,
        out_shape=out_shape,
    )(index, *operands)


def weight_kernel(index, gate, up, partner_gate, partner_up, blocks):
    count, _, width = blocks.shape
    units = gate.shape[0]
    for j in range(count):
        at = lanes(index[0, j], width)
        for i, source in enumerate((gate, up, partner_gate, partner_up)):
            blocks[j, i * units : (i + 1) * units] = source[:, at]


def project_kernel(index, group, hidden, proj, down, own, out):
    rows = group.shape[0]
    count, _, width = own.shape
    for side, to in ((1, out), (0, own)):
        for j in range(count):
            at = lanes(index[side, j], width)
            to[j, :rows] = jnp.dot(group[...], proj[:, at], preferred_element_type=f32).astype(bf16)
            to[j, rows:] = jnp.dot(hidden[...], down[:, at], preferred_element_type=f32).astype(bf16)


def after(x, event):
    return lax.optimization_barrier((x, event))[0]


def pool_group_out(pool_input, earlier_rows, pool_map, pool_scale, tp_rank, ep_rank):
    row_count, channels = pool_input.shape
    group_dim = pool_map.shape[1]
    local_groups = channels // group_dim
    values = pool_input.astype(f32)
    extended = jnp.concatenate([earlier_rows.astype(f32), values], axis=0)
    position = (ep_rank * row_count + jnp.arange(row_count, dtype=jnp.int32)).astype(f32)
    group_ids = tp_rank * local_groups + jnp.arange(channels, dtype=jnp.int32) // group_dim
    group_kind = group_ids % 4
    running = jnp.zeros((row_count, channels), f32)
    pooled = -values
    for lag_step in range(reach_back + 1):
        running = running + extended[reach_back - lag_step : reach_back - lag_step + row_count]
        if lag_step + 1 in windows:
            kind_id = windows.index(lag_step + 1)
            counts = jnp.minimum(position + 1.0, float(lag_step + 1))
            select = (group_kind == kind_id).astype(f32)
            pooled = pooled + select[None, :] * running / counts[:, None]
    pooled = pooled.astype(bf16)
    my_maps = lax.dynamic_slice_in_dim(pool_map, tp_rank * local_groups, local_groups, 0)
    my_scale = lax.dynamic_slice_in_dim(pool_scale, tp_rank * channels, channels, 0)
    mapped = jnp.einsum(
        "rgc,gcd->rgd",
        pooled.reshape(row_count, local_groups, group_dim),
        my_maps,
        preferred_element_type=f32,
    )
    return (mapped.reshape(row_count, channels) * my_scale[None, :]).astype(bf16)


def per_device(
    pool_input,
    pool_map,
    pool_scale,
    out_proj,
    moe_input,
    norm_gain,
    routes,
    route_weights,
    expert_gate,
    expert_up,
    expert_down,
    shared_gate,
    shared_up,
    shared_down,
):
    tp_rank = lax.axis_index("tp")
    ep_rank = lax.axis_index("ep")
    tp_size = lax.axis_size("tp")
    expert_count = lax.axis_size("ep")
    y_size = tp_size // 2
    core = tp_rank % 2
    y = tp_rank // 2
    tok_count, width = moe_input.shape
    top_count = routes.shape[1]
    capacity = (3 * tok_count * top_count + 2 * expert_count - 1) // (2 * expert_count)
    buffer_len = expert_count * capacity
    slice_width = width // tp_size
    row_count = pool_input.shape[0]

    earlier_rows = halo(pool_input[row_count - reach_back :])

    routes_t = routes.T
    experts = jnp.arange(expert_count, dtype=jnp.int32)[:, None]
    named = jnp.zeros((expert_count, tok_count), f32)
    weight_t = jnp.zeros((expert_count, tok_count), f32)
    for k in range(top_count):
        hit = routes_t[k][None, :] == experts
        named = named + hit.astype(f32)
        weight_t = weight_t + jnp.where(hit, route_weights.T[k][None, :], 0.0)
    before = jnp.arange(tok_count)[:, None] < jnp.arange(tok_count)[None, :]
    earlier = jnp.dot(named.astype(bf16), before.astype(bf16), preferred_element_type=f32)
    slot = jnp.where(named > 0, earlier, -1.0)
    slots = jnp.arange(capacity, dtype=f32)[None, :, None]
    match = slot[:, None, :] == slots
    placing = match.astype(bf16).reshape(buffer_len, tok_count)
    combine = jnp.where(match, weight_t[:, None, :], 0.0).astype(bf16).reshape(buffer_len, tok_count)

    values = moe_input.astype(f32)
    mean = jnp.mean(values, axis=1, keepdims=True)
    centre = values - mean
    rstd = lax.rsqrt(jnp.mean(centre * centre, axis=1, keepdims=True) + eps)

    def normed_slice(far):
        at = (((y + far) % y_size) * 2 + core) * slice_width
        mine = lax.dynamic_slice_in_dim(moe_input, at, slice_width, 1).astype(f32)
        gain = lax.dynamic_slice_in_dim(norm_gain, at, slice_width, 0)
        return ((mine - mean) * rstd * gain[None, :]).astype(bf16)

    def exchanged(rows):
        return lax.all_to_all(rows, "ep", split_axis=0, concat_axis=0, tiled=True)

    both = jnp.concatenate([normed_slice(0), normed_slice(y_size // 2)], axis=1)
    outgoing = jnp.dot(placing, both, preferred_element_type=f32).astype(bf16)
    arrived = exchanged(outgoing)
    pool_input = after(pool_input, outgoing)
    turn = (y + jnp.arange(y_size, dtype=jnp.int32)) % y_size
    index = jnp.stack([turn * 2 + core, turn * 2 + 1 - core]).astype(jnp.int32)

    group_out = pool_group_out(pool_input, earlier_rows, pool_map, pool_scale, tp_rank, ep_rank)
    normed = (centre * rstd * norm_gain[None, :]).astype(bf16)
    shared_gate_val = jnp.dot(normed, shared_gate, preferred_element_type=f32)
    shared_up_val = jnp.dot(normed, shared_up, preferred_element_type=f32)
    shared_hidden = (jax.nn.silu(shared_gate_val) * shared_up_val).astype(bf16)

    shape = jax.ShapeDtypeStruct((y_size, row_count + tok_count, slice_width), bf16)
    kept, sent = local_kernel(project_kernel, index, (group_out, shared_hidden, out_proj, shared_down), [shape, shape])
    from_partner = to_partner(sent)


    gate_t = expert_gate[0].T
    up_t = expert_up[0].T
    units = gate_t.shape[0]
    blocks = jax.ShapeDtypeStruct((y_size, 4 * units, slice_width), bf16)
    weights = local_kernel(weight_kernel, index, (gate_t, up_t, to_partner(gate_t), to_partner(up_t)), blocks)

    def part(j):
        return kept[j].astype(f32) + from_partner[j].astype(f32)

    def reduced(rs_up, rs_down, step):
        rs_up = (part(4 - step) + rs_up.astype(f32)).astype(bf16)
        rs_down = (part(5 + step) + rs_down.astype(f32)).astype(bf16)
        rs_up, rs_down = lax.optimization_barrier((rs_up, rs_down))
        return along_y(rs_up, 1), along_y(rs_down, -1)

    arrived = after(arrived, (from_partner, weights))
    near = arrived[:, :slice_width]
    far = arrived[:, slice_width:]

    def product(rows, j):
        return tdot(weights[j % y_size], rows)

    up = along_y(near, 1)
    down = along_y(near, -1)
    up_far = along_y(far, 1)
    down_far = along_y(far, -1)
    up_two = along_y(up, 1)
    down_two = along_y(down, -1)
    rs_up = along_y(part(4).astype(bf16), 1)
    rs_down = along_y(part(5).astype(bf16), -1)
    rs_up, rs_down = lax.optimization_barrier((rs_up, rs_down))
    rs_up, rs_down = reduced(rs_up, rs_down, 1)
    summed = product(near, 0) + product(far, 4)
    summed = summed + product(up, -1) + product(down, 1)
    summed = summed + product(up_far, 3) + product(down_far, -3)
    summed = summed + product(up_two, -2) + product(down_two, 2)
    full = summed[: 2 * units] + to_partner(summed[2 * units :])
    hidden = (jax.nn.silu(full[:units]) * full[units:]).astype(bf16)


    copies = jnp.broadcast_to(hidden[None], (y_size, *hidden.shape))
    groups = [[2 * i + c for i in range(y_size)] for c in range(2)]
    own_hidden = lax.all_to_all(copies, "tp", 0, 0, axis_index_groups=groups, tiled=True)
    rs_up, rs_down = after((rs_up, rs_down), own_hidden)
    rs_up, rs_down = reduced(rs_up, rs_down, 2)
    other_hidden = to_partner(own_hidden)
    down_weight = expert_down[0].reshape(y_size, 2, units, slice_width)

    def down_product(h, side):
        w = lax.dynamic_index_in_dim(down_weight, side, 1, keepdims=False)
        w = w.reshape(y_size * units, slice_width)
        return lax.dot_general(
            h.reshape(y_size * units, buffer_len), w, (((0,), (0,)), ((), ())), preferred_element_type=f32
        )

    expert_result = down_product(own_hidden, core) + down_product(other_hidden, 1 - core)
    expert_result = expert_result.astype(bf16)
    returned = exchanged(expert_result)
    rs_up = along_y((part(1) + rs_up.astype(f32)).astype(bf16), 1)
    routed = lax.dot_general(combine, returned, (((0,), (0,)), ((), ())), preferred_element_type=f32)

    total = part(0) + rs_up.astype(f32) + rs_down.astype(f32)
    return (total[:row_count].astype(bf16), (routed + total[row_count:]).astype(bf16))


def solution(mesh):
    return jax.shard_map(
        per_device,
        mesh=mesh,
        in_specs=(
            P("ep", "tp"),
            P(),
            P(),
            P("tp", None),
            P("ep", None),
            P(),
            P("ep", None),
            P("ep", None),
            P("ep", None, "tp"),
            P("ep", None, "tp"),
            P("ep", None, "tp"),
            P(None, "tp"),
            P(None, "tp"),
            P("tp", None),
        ),
        out_specs=(P("ep", "tp"), P("ep", "tp")),
        check_vma=False,
    )
```

```python
import jax
import jax.numpy as jnp
from jax import lax
from jax.experimental import pallas as pl
from jax.experimental.pallas import tpu as pltpu
from jax.sharding import PartitionSpec as P


windows = (2, 4, 8, 16)
reach_back = 15
eps = 1e-05
f32 = jnp.float32
bf16 = jnp.bfloat16


def halo(block):
    devices = range(lax.axis_size("ep"))
    return lax.ppermute(block, "ep", [(i - 1, i) for i in devices if i > 0])


def along_y(x, step):
    n = lax.axis_size("tp")
    return lax.ppermute(x, "tp", [(i, (i + 2 * step) % n) for i in range(n)])


def to_partner(x):
    n = lax.axis_size("tp")
    return lax.ppermute(x, "tp", [(i, i ^ 1) for i in range(n)])


def tdot(a, b):
    return lax.dot_general(a, b, (((1,), (1,)), ((), ())), preferred_element_type=f32)


def lanes(block, width):
    return pl.ds(pl.multiple_of(block * width, width), width)


def local_kernel(body, index, operands, out_shape):
    vmem = pl.BlockSpec(memory_space=pltpu.VMEM)
    smem = pl.BlockSpec(memory_space=pltpu.SMEM)
    several = isinstance(out_shape, list)
    return pl.pallas_call(
        body,
        in_specs=[smem] + [vmem] * len(operands),
        out_specs=[vmem] * len(out_shape) if several else vmem,
        out_shape=out_shape,
    )(index, *operands)


def weight_kernel(index, gate, up, partner_gate, partner_up, blocks):
    count, _, width = blocks.shape
    units = gate.shape[0]
    for j in range(count):
        at = lanes(index[0, j], width)
        for i, source in enumerate((gate, up, partner_gate, partner_up)):
            blocks[j, i * units : (i + 1) * units] = source[:, at]


def project_kernel(index, group, hidden, proj, down, own, out):
    rows = group.shape[0]
    count, _, width = own.shape
    for side, to in ((1, out), (0, own)):
        for j in range(count):
            at = lanes(index[side, j], width)
            to[j, :rows] = jnp.dot(group[...], proj[:, at], preferred_element_type=f32).astype(bf16)
            to[j, rows:] = jnp.dot(hidden[...], down[:, at], preferred_element_type=f32).astype(bf16)


def after(x, event):
    return lax.optimization_barrier((x, event))[0]


def pool_group_out(pool_input, earlier_rows, pool_map, pool_scale, tp_rank, ep_rank):
    row_count, channels = pool_input.shape
    group_dim = pool_map.shape[1]
    local_groups = channels // group_dim
    values = pool_input.astype(f32)
    extended = jnp.concatenate([earlier_rows.astype(f32), values], axis=0)
    position = (ep_rank * row_count + jnp.arange(row_count, dtype=jnp.int32)).astype(f32)
    group_ids = tp_rank * local_groups + jnp.arange(channels, dtype=jnp.int32) // group_dim
    group_kind = group_ids % 4
    running = jnp.zeros((row_count, channels), f32)
    pooled = -values
    for lag_step in range(reach_back + 1):
        running = running + extended[reach_back - lag_step : reach_back - lag_step + row_count]
        if lag_step + 1 in windows:
            kind_id = windows.index(lag_step + 1)
            counts = jnp.minimum(position + 1.0, float(lag_step + 1))
            select = (group_kind == kind_id).astype(f32)
            pooled = pooled + select[None, :] * running / counts[:, None]
    pooled = pooled.astype(bf16)
    my_maps = lax.dynamic_slice_in_dim(pool_map, tp_rank * local_groups, local_groups, 0)
    my_scale = lax.dynamic_slice_in_dim(pool_scale, tp_rank * channels, channels, 0)
    mapped = jnp.einsum(
        "rgc,gcd->rgd",
        pooled.reshape(row_count, local_groups, group_dim),
        my_maps,
        preferred_element_type=f32,
    )
    return (mapped.reshape(row_count, channels) * my_scale[None, :]).astype(bf16)


def per_device(
    pool_input,
    pool_map,
    pool_scale,
    out_proj,
    moe_input,
    norm_gain,
    routes,
    route_weights,
    expert_gate,
    expert_up,
    expert_down,
    shared_gate,
    shared_up,
    shared_down,
):
    tp_rank = lax.axis_index("tp")
    ep_rank = lax.axis_index("ep")
    tp_size = lax.axis_size("tp")
    expert_count = lax.axis_size("ep")
    y_size = tp_size // 2
    core = tp_rank % 2
    y = tp_rank // 2
    tok_count, width = moe_input.shape
    top_count = routes.shape[1]
    capacity = (3 * tok_count * top_count + 2 * expert_count - 1) // (2 * expert_count)
    buffer_len = expert_count * capacity
    slice_width = width // tp_size
    row_count = pool_input.shape[0]

    earlier_rows = halo(pool_input[row_count - reach_back :])

    routes_t = routes.T
    experts = jnp.arange(expert_count, dtype=jnp.int32)[:, None]
    named = jnp.zeros((expert_count, tok_count), f32)
    weight_t = jnp.zeros((expert_count, tok_count), f32)
    for k in range(top_count):
        hit = routes_t[k][None, :] == experts
        named = named + hit.astype(f32)
        weight_t = weight_t + jnp.where(hit, route_weights.T[k][None, :], 0.0)
    before = jnp.arange(tok_count)[:, None] < jnp.arange(tok_count)[None, :]
    earlier = jnp.dot(named.astype(bf16), before.astype(bf16), preferred_element_type=f32)
    slot = jnp.where(named > 0, earlier, -1.0)
    slots = jnp.arange(capacity, dtype=f32)[None, :, None]
    match = slot[:, None, :] == slots
    placing = match.astype(bf16).reshape(buffer_len, tok_count)
    combine = jnp.where(match, weight_t[:, None, :], 0.0).astype(bf16).reshape(buffer_len, tok_count)

    values = moe_input.astype(f32)
    mean = jnp.mean(values, axis=1, keepdims=True)
    centre = values - mean
    rstd = lax.rsqrt(jnp.mean(centre * centre, axis=1, keepdims=True) + eps)

    def normed_slice(far):
        at = (((y + far) % y_size) * 2 + core) * slice_width
        mine = lax.dynamic_slice_in_dim(moe_input, at, slice_width, 1).astype(f32)
        gain = lax.dynamic_slice_in_dim(norm_gain, at, slice_width, 0)
        return ((mine - mean) * rstd * gain[None, :]).astype(bf16)

    def exchanged(rows):
        return lax.all_to_all(rows, "ep", split_axis=0, concat_axis=0, tiled=True)

    both = jnp.concatenate([normed_slice(0), normed_slice(y_size // 2)], axis=1)
    outgoing = jnp.dot(placing, both, preferred_element_type=f32).astype(bf16)
    arrived = exchanged(outgoing)
    pool_input = after(pool_input, outgoing)
    turn = (y + jnp.arange(y_size, dtype=jnp.int32)) % y_size
    index = jnp.stack([turn * 2 + core, turn * 2 + 1 - core]).astype(jnp.int32)

    group_out = pool_group_out(pool_input, earlier_rows, pool_map, pool_scale, tp_rank, ep_rank)
    normed = (centre * rstd * norm_gain[None, :]).astype(bf16)
    shared_gate_val = jnp.dot(normed, shared_gate, preferred_element_type=f32)
    shared_up_val = jnp.dot(normed, shared_up, preferred_element_type=f32)
    shared_hidden = (jax.nn.silu(shared_gate_val) * shared_up_val).astype(bf16)

    shape = jax.ShapeDtypeStruct((y_size, row_count + tok_count, slice_width), bf16)
    kept, sent = local_kernel(project_kernel, index, (group_out, shared_hidden, out_proj, shared_down), [shape, shape])
    from_partner = to_partner(sent)


    gate_t = expert_gate[0].T
    up_t = expert_up[0].T
    units = gate_t.shape[0]
    blocks = jax.ShapeDtypeStruct((y_size, 4 * units, slice_width), bf16)
    partner_gate = to_partner(gate_t)
    partner_up = to_partner(up_t)
    weights = local_kernel(weight_kernel, index, (gate_t, up_t, partner_gate, partner_up), blocks)

    def part(j):
        return kept[j].astype(f32) + from_partner[j].astype(f32)

    def reduced(rs_up, rs_down, step):
        rs_up = (part(4 - step) + rs_up.astype(f32)).astype(bf16)
        rs_down = (part(5 + step) + rs_down.astype(f32)).astype(bf16)
        rs_up, rs_down = lax.optimization_barrier((rs_up, rs_down))
        return along_y(rs_up, 1), along_y(rs_down, -1)

    near = arrived[:, :slice_width]
    far = arrived[:, slice_width:]

    def product(rows, j):
        return tdot(weights[j % y_size], rows)

    up = along_y(near, 1)
    down = along_y(near, -1)
    up_far = along_y(far, 1)
    down_far = along_y(far, -1)
    up_two = along_y(up, 1)
    down_two = along_y(down, -1)
    rs_up = along_y(part(4).astype(bf16), 1)
    rs_down = along_y(part(5).astype(bf16), -1)
    rs_up, rs_down = lax.optimization_barrier((rs_up, rs_down))
    rs_up, rs_down = reduced(rs_up, rs_down, 1)
    summed = product(near, 0) + product(far, 4)
    summed = summed + product(up, -1) + product(down, 1)
    summed = summed + product(up_far, 3) + product(down_far, -3)
    summed = summed + product(up_two, -2) + product(down_two, 2)
    full = summed[: 2 * units] + to_partner(summed[2 * units :])
    hidden = (jax.nn.silu(full[:units]) * full[units:]).astype(bf16)


    copies = jnp.broadcast_to(hidden[None], (y_size, *hidden.shape))
    groups = [[2 * i + c for i in range(y_size)] for c in range(2)]
    own_hidden = lax.all_to_all(copies, "tp", 0, 0, axis_index_groups=groups, tiled=True)
    rs_up, rs_down = reduced(rs_up, rs_down, 2)
    other_hidden = to_partner(own_hidden)
    down_weight = expert_down[0].reshape(y_size, 2, units, slice_width)

    def down_product(h, side):
        w = lax.dynamic_index_in_dim(down_weight, side, 1, keepdims=False)
        w = w.reshape(y_size * units, slice_width)
        return lax.dot_general(
            h.reshape(y_size * units, buffer_len), w, (((0,), (0,)), ((), ())), preferred_element_type=f32
        )

    expert_result = down_product(own_hidden, core) + down_product(other_hidden, 1 - core)
    expert_result = expert_result.astype(bf16)
    returned = exchanged(expert_result)
    rs_up = along_y((part(1) + rs_up.astype(f32)).astype(bf16), 1)
    routed = lax.dot_general(combine, returned, (((0,), (0,)), ((), ())), preferred_element_type=f32)

    total = part(0) + rs_up.astype(f32) + rs_down.astype(f32)
    return (total[:row_count].astype(bf16), (routed + total[row_count:]).astype(bf16))


def solution(mesh):
    return jax.shard_map(
        per_device,
        mesh=mesh,
        in_specs=(
            P("ep", "tp"),
            P(),
            P(),
            P("tp", None),
            P("ep", None),
            P(),
            P("ep", None),
            P("ep", None),
            P("ep", None, "tp"),
            P("ep", None, "tp"),
            P("ep", None, "tp"),
            P(None, "tp"),
            P(None, "tp"),
            P("tp", None),
        ),
        out_specs=(P("ep", "tp"), P("ep", "tp")),
        check_vma=False,
    )
```

```python
import jax
import jax.numpy as jnp
from jax import lax
from jax.experimental import pallas as pl
from jax.experimental.pallas import tpu as pltpu
from jax.sharding import PartitionSpec as P


windows = (2, 4, 8, 16)
reach_back = 15
eps = 1e-05
f32 = jnp.float32
bf16 = jnp.bfloat16


def halo(block):
    devices = range(lax.axis_size("ep"))
    return lax.ppermute(block, "ep", [(i - 1, i) for i in devices if i > 0])


def sent(x, targets):
    n = lax.axis_size("tp") // 2
    route = []
    for core, (step, to) in targets.items():
        route += [(2 * i + core, 2 * ((i + step) % n) + to) for i in range(n)]
    return lax.ppermute(x, "tp", route)


def to_partner(x):
    n = lax.axis_size("tp")
    return lax.ppermute(x, "tp", [(i, i ^ 1) for i in range(n)])


def tdot(a, b):
    return lax.dot_general(a, b, (((1,), (1,)), ((), ())), preferred_element_type=f32)


def lanes(block, width):
    return pl.ds(pl.multiple_of(block * width, width), width)


def local_kernel(body, index, operands, out_shape):
    vmem = pl.BlockSpec(memory_space=pltpu.VMEM)
    smem = pl.BlockSpec(memory_space=pltpu.SMEM)
    several = isinstance(out_shape, list)
    return pl.pallas_call(
        body,
        in_specs=[smem] + [vmem] * len(operands),
        out_specs=[vmem] * len(out_shape) if several else vmem,
        out_shape=out_shape,
    )(index, *operands)


def weight_kernel(index, gate, up, partner_gate, partner_up, blocks):
    count, _, width = blocks.shape
    units = gate.shape[0]
    for j in range(count):
        at = lanes(index[j], width)
        for i, source in enumerate((gate, up, partner_gate, partner_up)):
            blocks[j, i * units : (i + 1) * units] = source[:, at]


def project_kernel(index, group, hidden, proj, down, own, out):
    rows = group.shape[0]
    count, _, width = own.shape
    for side, to in ((1, out), (0, own)):
        for j in range(count):
            at = lanes(index[side, j], width)
            to[j, :rows] = jnp.dot(group[...], proj[:, at], preferred_element_type=f32).astype(bf16)
            to[j, rows:] = jnp.dot(hidden[...], down[:, at], preferred_element_type=f32).astype(bf16)


def after(x, event):
    return lax.optimization_barrier((x, event))[0]


def pool_group_out(pool_input, earlier_rows, pool_map, pool_scale, tp_rank, ep_rank):
    row_count, channels = pool_input.shape
    group_dim = pool_map.shape[1]
    local_groups = channels // group_dim
    values = pool_input.astype(f32)
    extended = jnp.concatenate([earlier_rows.astype(f32), values], axis=0)
    position = (ep_rank * row_count + jnp.arange(row_count, dtype=jnp.int32)).astype(f32)
    group_ids = tp_rank * local_groups + jnp.arange(channels, dtype=jnp.int32) // group_dim
    group_kind = group_ids % 4
    running = jnp.zeros((row_count, channels), f32)
    pooled = -values
    for lag_step in range(reach_back + 1):
        running = running + extended[reach_back - lag_step : reach_back - lag_step + row_count]
        if lag_step + 1 in windows:
            kind_id = windows.index(lag_step + 1)
            counts = jnp.minimum(position + 1.0, float(lag_step + 1))
            select = (group_kind == kind_id).astype(f32)
            pooled = pooled + select[None, :] * running / counts[:, None]
    pooled = pooled.astype(bf16)
    my_maps = lax.dynamic_slice_in_dim(pool_map, tp_rank * local_groups, local_groups, 0)
    my_scale = lax.dynamic_slice_in_dim(pool_scale, tp_rank * channels, channels, 0)
    mapped = jnp.einsum(
        "rgc,gcd->rgd",
        pooled.reshape(row_count, local_groups, group_dim),
        my_maps,
        preferred_element_type=f32,
    )
    return (mapped.reshape(row_count, channels) * my_scale[None, :]).astype(bf16)


def per_device(
    pool_input,
    pool_map,
    pool_scale,
    out_proj,
    moe_input,
    norm_gain,
    routes,
    route_weights,
    expert_gate,
    expert_up,
    expert_down,
    shared_gate,
    shared_up,
    shared_down,
):
    tp_rank = lax.axis_index("tp")
    ep_rank = lax.axis_index("ep")
    tp_size = lax.axis_size("tp")
    expert_count = lax.axis_size("ep")
    y_size = tp_size // 2
    core = tp_rank % 2
    y = tp_rank // 2
    tok_count, width = moe_input.shape
    top_count = routes.shape[1]
    capacity = (3 * tok_count * top_count + 2 * expert_count - 1) // (2 * expert_count)
    buffer_len = expert_count * capacity
    slice_width = width // tp_size
    row_count = pool_input.shape[0]

    earlier_rows = halo(pool_input[row_count - reach_back :])

    routes_t = routes.T
    experts = jnp.arange(expert_count, dtype=jnp.int32)[:, None]
    named = jnp.zeros((expert_count, tok_count), f32)
    weight_t = jnp.zeros((expert_count, tok_count), f32)
    for k in range(top_count):
        hit = routes_t[k][None, :] == experts
        named = named + hit.astype(f32)
        weight_t = weight_t + jnp.where(hit, route_weights.T[k][None, :], 0.0)
    before = jnp.arange(tok_count)[:, None] < jnp.arange(tok_count)[None, :]
    earlier = jnp.dot(named.astype(bf16), before.astype(bf16), preferred_element_type=f32)
    slot = jnp.where(named > 0, earlier, -1.0)
    slots = jnp.arange(capacity, dtype=f32)[None, :, None]
    match = slot[:, None, :] == slots
    placing = match.astype(bf16).reshape(buffer_len, tok_count)
    combine = jnp.where(match, weight_t[:, None, :], 0.0).astype(bf16).reshape(buffer_len, tok_count)

    values = moe_input.astype(f32)
    mean = jnp.mean(values, axis=1, keepdims=True)
    centre = values - mean
    rstd = lax.rsqrt(jnp.mean(centre * centre, axis=1, keepdims=True) + eps)

    home = y + core * (y_size // 2)
    chip_width = 2 * slice_width
    at = (home % y_size) * chip_width
    mine = lax.dynamic_slice_in_dim(moe_input, at, chip_width, 1).astype(f32)
    gain = lax.dynamic_slice_in_dim(norm_gain, at, chip_width, 0)
    normed_slice = ((mine - mean) * rstd * gain[None, :]).astype(bf16)

    def exchanged(rows):
        return lax.all_to_all(rows, "ep", split_axis=0, concat_axis=0, tiled=True)

    outgoing = jnp.dot(placing, normed_slice, preferred_element_type=f32).astype(bf16)
    arrived = exchanged(outgoing)
    pool_input = after(pool_input, outgoing)
    upward = jnp.array([4, 3, 2, 1], jnp.int32)
    downward = jnp.array([5, 6, 7, 0], jnp.int32)
    kept_ids = jnp.where(core == 0, upward, downward)
    sent_ids = jnp.where(core == 0, downward, upward)
    index = (y + jnp.stack([kept_ids, sent_ids])) % y_size
    near_index = (home + y_size + jnp.array([0, -1, 1, -2, 2], jnp.int32)) % y_size

    group_out = pool_group_out(pool_input, earlier_rows, pool_map, pool_scale, tp_rank, ep_rank)
    normed = (centre * rstd * norm_gain[None, :]).astype(bf16)
    shared_gate_val = jnp.dot(normed, shared_gate, preferred_element_type=f32)
    shared_up_val = jnp.dot(normed, shared_up, preferred_element_type=f32)
    shared_hidden = (jax.nn.silu(shared_gate_val) * shared_up_val).astype(bf16)

    shape = jax.ShapeDtypeStruct((y_size // 2, row_count + tok_count, chip_width), bf16)
    kept, given = local_kernel(project_kernel, index, (group_out, shared_hidden, out_proj, shared_down), [shape, shape])
    from_partner = to_partner(given)

    gate_t = expert_gate[0].T
    up_t = expert_up[0].T
    units = gate_t.shape[0]
    blocks = jax.ShapeDtypeStruct((5, 4 * units, chip_width), bf16)
    partner_gate = to_partner(gate_t)
    partner_up = to_partner(up_t)
    weights = local_kernel(weight_kernel, near_index, (gate_t, up_t, partner_gate, partner_up), blocks)

    def part(j):
        return kept[j].astype(f32) + from_partner[j].astype(f32)

    def ring_step(x):
        return sent(x.astype(bf16), {0: (1, 0), 1: (-1, 1)})

    up = sent(arrived, {0: (1, 0), 1: (1, 1)})
    down = sent(arrived, {0: (-1, 0), 1: (-1, 1)})
    up_two = sent(up, {0: (1, 0)})
    down_two = sent(down, {0: (-1, 0)})
    ring = ring_step(part(0))
    ring = ring_step(part(1) + ring.astype(f32))
    summed = tdot(weights[0], arrived)
    for j, rows in enumerate((up, down, up_two, down_two)):
        summed = summed + tdot(weights[j + 1], rows)
    full = summed[: 2 * units] + to_partner(summed[2 * units :])
    hidden = (jax.nn.silu(full[:units]) * full[units:]).astype(bf16)


    copies = jnp.broadcast_to(hidden[None], (y_size, *hidden.shape))
    groups = [[2 * i + c for i in range(y_size)] for c in range(2)]
    own_hidden = lax.all_to_all(copies, "tp", 0, 0, axis_index_groups=groups, tiled=True)
    ring = ring_step(part(2) + ring.astype(f32))
    other_hidden = to_partner(own_hidden)
    down_weight = expert_down[0].reshape(y_size, 2, units, slice_width)

    def down_product(h, side):
        w = lax.dynamic_index_in_dim(down_weight, side, 1, keepdims=False)
        w = w.reshape(y_size * units, slice_width)
        return lax.dot_general(
            h.reshape(y_size * units, buffer_len), w, (((0,), (0,)), ((), ())), preferred_element_type=f32
        )

    expert_result = down_product(own_hidden, core) + down_product(other_hidden, 1 - core)
    expert_result = expert_result.astype(bf16)
    returned = exchanged(expert_result)
    routed = lax.dot_general(combine, returned, (((0,), (0,)), ((), ())), preferred_element_type=f32)

    done = part(3) + ring.astype(f32)
    low = done[:, :slice_width]
    high = done[:, slice_width:]
    cross = sent(jnp.where(core == 0, high, low).astype(bf16), {0: (1, 1), 1: (0, 0)})
    straight = sent(low.astype(bf16), {0: (1, 0)})
    total = cross.astype(f32) + straight.astype(f32) + jnp.where(core == 0, 0.0, high)
    return (total[:row_count].astype(bf16), (routed + total[row_count:]).astype(bf16))


def solution(mesh):
    return jax.shard_map(
        per_device,
        mesh=mesh,
        in_specs=(
            P("ep", "tp"),
            P(),
            P(),
            P("tp", None),
            P("ep", None),
            P(),
            P("ep", None),
            P("ep", None),
            P("ep", None, "tp"),
            P("ep", None, "tp"),
            P("ep", None, "tp"),
            P(None, "tp"),
            P(None, "tp"),
            P("tp", None),
        ),
        out_specs=(P("ep", "tp"), P("ep", "tp")),
        check_vma=False,
    )
```

```python
import jax
import jax.numpy as jnp
from jax import lax
from jax.experimental import pallas as pl
from jax.experimental.pallas import tpu as pltpu
from jax.sharding import PartitionSpec as P


windows = (2, 4, 8, 16)
reach_back = 15
eps = 1e-05
f32 = jnp.float32
bf16 = jnp.bfloat16


def halo(block):
    devices = range(lax.axis_size("ep"))
    return lax.ppermute(block, "ep", [(i - 1, i) for i in devices if i > 0])


def sent(x, targets):
    n = lax.axis_size("tp") // 2
    route = []
    for core, (step, to) in targets.items():
        route += [(2 * i + core, 2 * ((i + step) % n) + to) for i in range(n)]
    return lax.ppermute(x, "tp", route)


def to_partner(x):
    n = lax.axis_size("tp")
    return lax.ppermute(x, "tp", [(i, i ^ 1) for i in range(n)])


def tdot(a, b):
    return lax.dot_general(a, b, (((1,), (1,)), ((), ())), preferred_element_type=f32)


def lanes(block, width):
    return pl.ds(pl.multiple_of(block * width, width), width)


def local_kernel(body, index, operands, out_shape):
    vmem = pl.BlockSpec(memory_space=pltpu.VMEM)
    smem = pl.BlockSpec(memory_space=pltpu.SMEM)
    several = isinstance(out_shape, list)
    return pl.pallas_call(
        body,
        in_specs=[smem] + [vmem] * len(operands),
        out_specs=[vmem] * len(out_shape) if several else vmem,
        out_shape=out_shape,
    )(index, *operands)


def weight_kernel(index, gate, up, partner_gate, partner_up, blocks):
    count, _, width = blocks.shape
    units = gate.shape[0]
    for j in range(count):
        at = lanes(index[j], width)
        for i, source in enumerate((gate, up, partner_gate, partner_up)):
            blocks[j, i * units : (i + 1) * units] = source[:, at]


def project_kernel(index, group, hidden, proj, down, own, out):
    rows = group.shape[0]
    count, _, width = own.shape
    for side, to in ((1, out), (0, own)):
        for j in range(count):
            at = lanes(index[side, j], width)
            to[j, :rows] = jnp.dot(group[...], proj[:, at], preferred_element_type=f32).astype(bf16)
            to[j, rows:] = jnp.dot(hidden[...], down[:, at], preferred_element_type=f32).astype(bf16)


def after(x, event):
    return lax.optimization_barrier((x, event))[0]


def pool_group_out(pool_input, earlier_rows, pool_map, pool_scale, tp_rank, ep_rank):
    row_count, channels = pool_input.shape
    group_dim = pool_map.shape[1]
    local_groups = channels // group_dim
    values = pool_input.astype(f32)
    extended = jnp.concatenate([earlier_rows.astype(f32), values], axis=0)
    position = (ep_rank * row_count + jnp.arange(row_count, dtype=jnp.int32)).astype(f32)
    group_ids = tp_rank * local_groups + jnp.arange(channels, dtype=jnp.int32) // group_dim
    group_kind = group_ids % 4
    running = jnp.zeros((row_count, channels), f32)
    pooled = -values
    for lag_step in range(reach_back + 1):
        running = running + extended[reach_back - lag_step : reach_back - lag_step + row_count]
        if lag_step + 1 in windows:
            kind_id = windows.index(lag_step + 1)
            counts = jnp.minimum(position + 1.0, float(lag_step + 1))
            select = (group_kind == kind_id).astype(f32)
            pooled = pooled + select[None, :] * running / counts[:, None]
    pooled = pooled.astype(bf16)
    my_maps = lax.dynamic_slice_in_dim(pool_map, tp_rank * local_groups, local_groups, 0)
    my_scale = lax.dynamic_slice_in_dim(pool_scale, tp_rank * channels, channels, 0)
    mapped = jnp.einsum(
        "rgc,gcd->rgd",
        pooled.reshape(row_count, local_groups, group_dim),
        my_maps,
        preferred_element_type=f32,
    )
    return (mapped.reshape(row_count, channels) * my_scale[None, :]).astype(bf16)


def per_device(
    pool_input,
    pool_map,
    pool_scale,
    out_proj,
    moe_input,
    norm_gain,
    routes,
    route_weights,
    expert_gate,
    expert_up,
    expert_down,
    shared_gate,
    shared_up,
    shared_down,
):
    tp_rank = lax.axis_index("tp")
    ep_rank = lax.axis_index("ep")
    tp_size = lax.axis_size("tp")
    expert_count = lax.axis_size("ep")
    y_size = tp_size // 2
    core = tp_rank % 2
    y = tp_rank // 2
    tok_count, width = moe_input.shape
    top_count = routes.shape[1]
    capacity = (3 * tok_count * top_count + 2 * expert_count - 1) // (2 * expert_count)
    buffer_len = expert_count * capacity
    slice_width = width // tp_size
    row_count = pool_input.shape[0]

    earlier_rows = halo(pool_input[row_count - reach_back :])

    routes_t = routes.T
    experts = jnp.arange(expert_count, dtype=jnp.int32)[:, None]
    named = jnp.zeros((expert_count, tok_count), f32)
    weight_t = jnp.zeros((expert_count, tok_count), f32)
    for k in range(top_count):
        hit = routes_t[k][None, :] == experts
        named = named + hit.astype(f32)
        weight_t = weight_t + jnp.where(hit, route_weights.T[k][None, :], 0.0)
    before = jnp.arange(tok_count)[:, None] < jnp.arange(tok_count)[None, :]
    earlier = jnp.dot(named.astype(bf16), before.astype(bf16), preferred_element_type=f32)
    slot = jnp.where(named > 0, earlier, -1.0)
    slots = jnp.arange(capacity, dtype=f32)[None, :, None]
    match = slot[:, None, :] == slots
    placing = match.astype(bf16).reshape(buffer_len, tok_count)
    combine = jnp.where(match, weight_t[:, None, :], 0.0).astype(bf16).reshape(buffer_len, tok_count)

    values = moe_input.astype(f32)
    mean = jnp.mean(values, axis=1, keepdims=True)
    centre = values - mean
    rstd = lax.rsqrt(jnp.mean(centre * centre, axis=1, keepdims=True) + eps)

    home = y + core * (y_size // 2)
    chip_width = 2 * slice_width
    at = (home % y_size) * chip_width
    mine = lax.dynamic_slice_in_dim(moe_input, at, chip_width, 1).astype(f32)
    gain = lax.dynamic_slice_in_dim(norm_gain, at, chip_width, 0)
    normed_slice = ((mine - mean) * rstd * gain[None, :]).astype(bf16)

    def exchanged(rows):
        return lax.all_to_all(rows, "ep", split_axis=0, concat_axis=0, tiled=True)

    outgoing = jnp.dot(placing, normed_slice, preferred_element_type=f32).astype(bf16)
    arrived = exchanged(outgoing)
    pool_input = after(pool_input, outgoing)
    upward = jnp.array([4, 3, 2, 1], jnp.int32)
    downward = jnp.array([5, 6, 7, 0], jnp.int32)
    kept_ids = jnp.where(core == 0, upward, downward)
    sent_ids = jnp.where(core == 0, downward, upward)
    index = (y + jnp.stack([kept_ids, sent_ids])) % y_size
    offsets = jnp.where(core == 0, jnp.array([0, -1, 1, -2, 2], jnp.int32), jnp.array([0, 1, -1, 0, 0], jnp.int32))
    near_index = (home + y_size + offsets) % y_size

    group_out = pool_group_out(pool_input, earlier_rows, pool_map, pool_scale, tp_rank, ep_rank)
    normed = (centre * rstd * norm_gain[None, :]).astype(bf16)
    shared_gate_val = jnp.dot(normed, shared_gate, preferred_element_type=f32)
    shared_up_val = jnp.dot(normed, shared_up, preferred_element_type=f32)
    shared_hidden = (jax.nn.silu(shared_gate_val) * shared_up_val).astype(bf16)

    shape = jax.ShapeDtypeStruct((y_size // 2, row_count + tok_count, chip_width), bf16)
    kept, given = local_kernel(project_kernel, index, (group_out, shared_hidden, out_proj, shared_down), [shape, shape])
    from_partner = to_partner(given)

    gate_t = expert_gate[0].T
    up_t = expert_up[0].T
    units = gate_t.shape[0]
    blocks = jax.ShapeDtypeStruct((5, 4 * units, chip_width), bf16)
    partner_gate = to_partner(gate_t)
    partner_up = to_partner(up_t)
    weights = local_kernel(weight_kernel, near_index, (gate_t, up_t, partner_gate, partner_up), blocks)

    def part(j):
        return kept[j].astype(f32) + from_partner[j].astype(f32)

    def ring_step(x):
        return sent(x.astype(bf16), {0: (1, 0), 1: (-1, 1)})

    one = sent(arrived, {0: (1, 0), 1: (-1, 1)})
    other = sent(arrived, {0: (-1, 0), 1: (1, 1)})
    up_two = sent(one, {0: (1, 0)})
    down_two = sent(other, {0: (-1, 0)})
    ring = ring_step(part(0))
    ring = ring_step(part(1) + ring.astype(f32))
    summed = tdot(weights[0], arrived)
    for j, rows in enumerate((one, other, up_two, down_two)):
        summed = summed + tdot(weights[j + 1], rows)
    full = summed[: 2 * units] + to_partner(summed[2 * units :])
    hidden = (jax.nn.silu(full[:units]) * full[units:]).astype(bf16)


    copies = jnp.broadcast_to(hidden[None], (y_size, *hidden.shape))
    groups = [[2 * i + c for i in range(y_size)] for c in range(2)]
    own_hidden = lax.all_to_all(copies, "tp", 0, 0, axis_index_groups=groups, tiled=True)
    ring = ring_step(part(2) + ring.astype(f32))
    other_hidden = to_partner(own_hidden)
    down_weight = expert_down[0].reshape(y_size, 2, units, slice_width)

    def down_product(h, side):
        w = lax.dynamic_index_in_dim(down_weight, side, 1, keepdims=False)
        w = w.reshape(y_size * units, slice_width)
        return lax.dot_general(
            h.reshape(y_size * units, buffer_len), w, (((0,), (0,)), ((), ())), preferred_element_type=f32
        )

    expert_result = down_product(own_hidden, core) + down_product(other_hidden, 1 - core)
    expert_result = expert_result.astype(bf16)
    returned = exchanged(expert_result)
    routed = lax.dot_general(combine, returned, (((0,), (0,)), ((), ())), preferred_element_type=f32)

    done = part(3) + ring.astype(f32)
    low = done[:, :slice_width]
    high = done[:, slice_width:]
    cross = sent(jnp.where(core == 0, high, low).astype(bf16), {0: (1, 1), 1: (0, 0)})
    straight = sent(low.astype(bf16), {0: (1, 0)})
    total = cross.astype(f32) + straight.astype(f32) + jnp.where(core == 0, 0.0, high)
    return (total[:row_count].astype(bf16), (routed + total[row_count:]).astype(bf16))


def solution(mesh):
    return jax.shard_map(
        per_device,
        mesh=mesh,
        in_specs=(
            P("ep", "tp"),
            P(),
            P(),
            P("tp", None),
            P("ep", None),
            P(),
            P("ep", None),
            P("ep", None),
            P("ep", None, "tp"),
            P("ep", None, "tp"),
            P("ep", None, "tp"),
            P(None, "tp"),
            P(None, "tp"),
            P("tp", None),
        ),
        out_specs=(P("ep", "tp"), P("ep", "tp")),
        check_vma=False,
    )
```

```python
import jax
import jax.numpy as jnp
from jax import lax
from jax.experimental import pallas as pl
from jax.experimental.pallas import tpu as pltpu
from jax.sharding import PartitionSpec as P


windows = (2, 4, 8, 16)
reach_back = 15
eps = 1e-05
f32 = jnp.float32
bf16 = jnp.bfloat16


def halo(block):
    devices = range(lax.axis_size("ep"))
    return lax.ppermute(block, "ep", [(i - 1, i) for i in devices if i > 0])


def sent(x, targets):
    n = lax.axis_size("tp") // 2
    route = []
    for core, (step, to) in targets.items():
        route += [(2 * i + core, 2 * ((i + step) % n) + to) for i in range(n)]
    return lax.ppermute(x, "tp", route)


def to_partner(x):
    n = lax.axis_size("tp")
    return lax.ppermute(x, "tp", [(i, i ^ 1) for i in range(n)])


def tdot(a, b):
    return lax.dot_general(a, b, (((1,), (1,)), ((), ())), preferred_element_type=f32)


def lanes(block, width):
    return pl.ds(pl.multiple_of(block * width, width), width)


def local_kernel(body, index, operands, out_shape):
    vmem = pl.BlockSpec(memory_space=pltpu.VMEM)
    smem = pl.BlockSpec(memory_space=pltpu.SMEM)
    several = isinstance(out_shape, list)
    return pl.pallas_call(
        body,
        in_specs=[smem] + [vmem] * len(operands),
        out_specs=[vmem] * len(out_shape) if several else vmem,
        out_shape=out_shape,
    )(index, *operands)


def weight_kernel(index, gate, up, partner_gate, partner_up, blocks):
    count, _, width = blocks.shape
    units = gate.shape[0]
    first = index[count] == 0
    for j in range(count):
        at = lanes(index[j], width)
        for i, (own, partner) in enumerate(((gate, partner_gate), (up, partner_up))):
            mine = own[:, at]
            other = partner[:, at]
            low = 2 * i * units
            blocks[j, low : low + units] = jnp.where(first, mine, other)
            blocks[j, low + units : low + 2 * units] = jnp.where(first, other, mine)


def project_kernel(index, group, hidden, proj, down, own, out):
    rows = group.shape[0]
    count, _, width = own.shape
    for side, to in ((1, out), (0, own)):
        for j in range(count):
            at = lanes(index[side, j], width)
            to[j, :rows] = jnp.dot(group[...], proj[:, at], preferred_element_type=f32).astype(bf16)
            to[j, rows:] = jnp.dot(hidden[...], down[:, at], preferred_element_type=f32).astype(bf16)


def after(x, event):
    return lax.optimization_barrier((x, event))[0]


def pool_group_out(pool_input, earlier_rows, pool_map, pool_scale, tp_rank, ep_rank):
    row_count, channels = pool_input.shape
    group_dim = pool_map.shape[1]
    local_groups = channels // group_dim
    values = pool_input.astype(f32)
    extended = jnp.concatenate([earlier_rows.astype(f32), values], axis=0)
    position = (ep_rank * row_count + jnp.arange(row_count, dtype=jnp.int32)).astype(f32)
    group_ids = tp_rank * local_groups + jnp.arange(channels, dtype=jnp.int32) // group_dim
    group_kind = group_ids % 4
    running = jnp.zeros((row_count, channels), f32)
    pooled = -values
    for lag_step in range(reach_back + 1):
        running = running + extended[reach_back - lag_step : reach_back - lag_step + row_count]
        if lag_step + 1 in windows:
            kind_id = windows.index(lag_step + 1)
            counts = jnp.minimum(position + 1.0, float(lag_step + 1))
            select = (group_kind == kind_id).astype(f32)
            pooled = pooled + select[None, :] * running / counts[:, None]
    pooled = pooled.astype(bf16)
    my_maps = lax.dynamic_slice_in_dim(pool_map, tp_rank * local_groups, local_groups, 0)
    my_scale = lax.dynamic_slice_in_dim(pool_scale, tp_rank * channels, channels, 0)
    mapped = jnp.einsum(
        "rgc,gcd->rgd",
        pooled.reshape(row_count, local_groups, group_dim),
        my_maps,
        preferred_element_type=f32,
    )
    return (mapped.reshape(row_count, channels) * my_scale[None, :]).astype(bf16)


def per_device(
    pool_input,
    pool_map,
    pool_scale,
    out_proj,
    moe_input,
    norm_gain,
    routes,
    route_weights,
    expert_gate,
    expert_up,
    expert_down,
    shared_gate,
    shared_up,
    shared_down,
):
    tp_rank = lax.axis_index("tp")
    ep_rank = lax.axis_index("ep")
    tp_size = lax.axis_size("tp")
    expert_count = lax.axis_size("ep")
    y_size = tp_size // 2
    core = tp_rank % 2
    y = tp_rank // 2
    tok_count, width = moe_input.shape
    top_count = routes.shape[1]
    capacity = (3 * tok_count * top_count + 2 * expert_count - 1) // (2 * expert_count)
    buffer_len = expert_count * capacity
    slice_width = width // tp_size
    row_count = pool_input.shape[0]

    earlier_rows = halo(pool_input[row_count - reach_back :])

    routes_t = routes.T
    experts = jnp.arange(expert_count, dtype=jnp.int32)[:, None]
    named = jnp.zeros((expert_count, tok_count), f32)
    weight_t = jnp.zeros((expert_count, tok_count), f32)
    for k in range(top_count):
        hit = routes_t[k][None, :] == experts
        named = named + hit.astype(f32)
        weight_t = weight_t + jnp.where(hit, route_weights.T[k][None, :], 0.0)
    before = jnp.arange(tok_count)[:, None] < jnp.arange(tok_count)[None, :]
    earlier = jnp.dot(named.astype(bf16), before.astype(bf16), preferred_element_type=f32)
    slot = jnp.where(named > 0, earlier, -1.0)
    slots = jnp.arange(capacity, dtype=f32)[None, :, None]
    match = slot[:, None, :] == slots
    placing = match.astype(bf16).reshape(buffer_len, tok_count)
    combine = jnp.where(match, weight_t[:, None, :], 0.0).astype(bf16).reshape(buffer_len, tok_count)

    values = moe_input.astype(f32)
    mean = jnp.mean(values, axis=1, keepdims=True)
    centre = values - mean
    rstd = lax.rsqrt(jnp.mean(centre * centre, axis=1, keepdims=True) + eps)

    home = y + core * (y_size // 2)
    chip_width = 2 * slice_width
    at = (home % y_size) * chip_width
    mine = lax.dynamic_slice_in_dim(moe_input, at, chip_width, 1).astype(f32)
    gain = lax.dynamic_slice_in_dim(norm_gain, at, chip_width, 0)
    normed_slice = ((mine - mean) * rstd * gain[None, :]).astype(bf16)

    def exchanged(rows):
        return lax.all_to_all(rows, "ep", split_axis=0, concat_axis=0, tiled=True)

    outgoing = jnp.dot(placing, normed_slice, preferred_element_type=f32).astype(bf16)
    arrived = exchanged(outgoing)
    pool_input = after(pool_input, outgoing)
    upward = jnp.array([4, 3, 2, 1], jnp.int32)
    downward = jnp.array([5, 6, 7, 0], jnp.int32)
    kept_ids = jnp.where(core == 0, upward, downward)
    sent_ids = jnp.where(core == 0, downward, upward)
    index = (y + jnp.stack([kept_ids, sent_ids])) % y_size
    offsets = jnp.where(core == 0, jnp.array([0, -1, 1, -2, 2], jnp.int32), jnp.array([0, 1, -1, 0, 0], jnp.int32))
    near_index = (home + y_size + offsets) % y_size
    near_index = jnp.concatenate([near_index, core[None]]).astype(jnp.int32)

    group_out = pool_group_out(pool_input, earlier_rows, pool_map, pool_scale, tp_rank, ep_rank)
    normed = (centre * rstd * norm_gain[None, :]).astype(bf16)
    shared_gate_val = jnp.dot(normed, shared_gate, preferred_element_type=f32)
    shared_up_val = jnp.dot(normed, shared_up, preferred_element_type=f32)
    shared_hidden = (jax.nn.silu(shared_gate_val) * shared_up_val).astype(bf16)

    shape = jax.ShapeDtypeStruct((y_size // 2, row_count + tok_count, chip_width), bf16)
    kept, given = local_kernel(project_kernel, index, (group_out, shared_hidden, out_proj, shared_down), [shape, shape])
    from_partner = to_partner(given)

    gate_t = expert_gate[0].T
    up_t = expert_up[0].T
    units = gate_t.shape[0]
    blocks = jax.ShapeDtypeStruct((5, 4 * units, chip_width), bf16)
    partner_gate = to_partner(gate_t)
    partner_up = to_partner(up_t)
    own_down = expert_down[0]
    partner_down = to_partner(own_down)
    weights = local_kernel(weight_kernel, near_index, (gate_t, up_t, partner_gate, partner_up), blocks)

    def part(j):
        return kept[j].astype(f32) + from_partner[j].astype(f32)

    def ring_sum(j, ring):
        return (part(j) + ring.astype(f32)).astype(bf16)

    def ring_step(x):
        return sent(x.astype(bf16), {0: (1, 0), 1: (-1, 1)})

    one = sent(arrived, {0: (1, 0), 1: (-1, 1)})
    other = sent(arrived, {0: (-1, 0), 1: (1, 1)})
    up_two = sent(one, {0: (1, 0)})
    down_two = sent(other, {0: (-1, 0)})
    ring = ring_step(part(0))
    ring = ring_step(ring_sum(1, ring))
    summed = tdot(weights[0], arrived)
    for j, rows in enumerate((one, other, up_two, down_two)):
        summed = summed + tdot(weights[j + 1], rows)
    full = summed + to_partner(summed)
    chip_units = 2 * units
    hidden = (jax.nn.silu(full[:chip_units]) * full[chip_units:]).astype(bf16)

    half = jnp.where(core == 0, hidden[:units], hidden[units:])
    pieces = [(half, 0, units)]
    for distance in range(y_size // 2, 0, -1):
        block = half if 2 * distance == y_size else hidden
        route = {0: (distance, 0), 1: (-distance, 1)}
        pieces.append((sent(block, route), distance, block.shape[0]))
    own_sum = partner_sum = 0.0
    for h, distance, rows in pieces:
        chip = (y + y_size + jnp.where(core == 0, -distance, distance)) % y_size
        begin = chip * chip_units + (core * units if rows == units else 0)

        def down_product(weight):
            w = lax.dynamic_slice_in_dim(weight, begin, rows, 0)
            return lax.dot_general(h, w, (((0,), (0,)), ((), ())), preferred_element_type=f32)

        own_sum = own_sum + down_product(own_down)
        partner_sum = partner_sum + down_product(partner_down)
    ring = ring_step(ring_sum(2, ring))
    expert_result = own_sum + to_partner(partner_sum.astype(bf16)).astype(f32)
    expert_result = expert_result.astype(bf16)
    returned = exchanged(expert_result)
    routed = lax.dot_general(combine, returned, (((0,), (0,)), ((), ())), preferred_element_type=f32)

    done = part(3) + ring.astype(f32)
    low = done[:, :slice_width]
    high = done[:, slice_width:]
    cross = sent(jnp.where(core == 0, high, low).astype(bf16), {0: (1, 1), 1: (0, 0)})
    straight = sent(low.astype(bf16), {0: (1, 0)})
    total = cross.astype(f32) + straight.astype(f32) + jnp.where(core == 0, 0.0, high)
    return (total[:row_count].astype(bf16), (routed + total[row_count:]).astype(bf16))


def solution(mesh):
    return jax.shard_map(
        per_device,
        mesh=mesh,
        in_specs=(
            P("ep", "tp"),
            P(),
            P(),
            P("tp", None),
            P("ep", None),
            P(),
            P("ep", None),
            P("ep", None),
            P("ep", None, "tp"),
            P("ep", None, "tp"),
            P("ep", None, "tp"),
            P(None, "tp"),
            P(None, "tp"),
            P("tp", None),
        ),
        out_specs=(P("ep", "tp"), P("ep", "tp")),
        check_vma=False,
    )
```

```python
import jax
import jax.numpy as jnp
from jax import lax
from jax.experimental import pallas as pl
from jax.experimental.pallas import tpu as pltpu
from jax.sharding import PartitionSpec as P


windows = (2, 4, 8, 16)
reach_back = 15
eps = 1e-05
f32 = jnp.float32
bf16 = jnp.bfloat16


def halo(block):
    devices = range(lax.axis_size("ep"))
    return lax.ppermute(block, "ep", [(i - 1, i) for i in devices if i > 0])


def sent(x, targets):
    n = lax.axis_size("tp") // 2
    route = []
    for core, (step, to) in targets.items():
        route += [(2 * i + core, 2 * ((i + step) % n) + to) for i in range(n)]
    return lax.ppermute(x, "tp", route)


def to_partner(x):
    n = lax.axis_size("tp")
    return lax.ppermute(x, "tp", [(i, i ^ 1) for i in range(n)])


def tdot(a, b):
    return lax.dot_general(a, b, (((1,), (1,)), ((), ())), preferred_element_type=f32)


def lanes(block, width):
    return pl.ds(pl.multiple_of(block * width, width), width)


def local_kernel(body, index, operands, out_shape):
    vmem = pl.BlockSpec(memory_space=pltpu.VMEM)
    smem = pl.BlockSpec(memory_space=pltpu.SMEM)
    several = isinstance(out_shape, list)
    return pl.pallas_call(
        body,
        in_specs=[smem] + [vmem] * len(operands),
        out_specs=[vmem] * len(out_shape) if several else vmem,
        out_shape=out_shape,
    )(index, *operands)


def weight_kernel(index, gate, up, partner_gate, partner_up, blocks):
    count, _, width = blocks.shape
    units = gate.shape[0]
    first = index[count] == 0
    for j in range(count):
        at = lanes(index[j], width)
        for i, (own, partner) in enumerate(((gate, partner_gate), (up, partner_up))):
            mine = own[:, at]
            other = partner[:, at]
            low = 2 * i * units
            blocks[j, low : low + units] = jnp.where(first, mine, other)
            blocks[j, low + units : low + 2 * units] = jnp.where(first, other, mine)


def project_kernel(index, group, hidden, proj, down, own, out):
    rows = group.shape[0]
    count, _, width = own.shape
    for side, to in ((1, out), (0, own)):
        for j in range(count):
            at = lanes(index[side, j], width)
            to[j, :rows] = jnp.dot(group[...], proj[:, at], preferred_element_type=f32).astype(bf16)
            to[j, rows:] = jnp.dot(hidden[...], down[:, at], preferred_element_type=f32).astype(bf16)


def down_kernel(index, *refs):
    *pieces, own, partner, own_sum, partner_sum = refs
    unit = pieces[0].shape[0]
    for weight, to in ((partner, partner_sum), (own, own_sum)):
        total = None
        for i, piece in enumerate(pieces):
            rows = pl.ds(pl.multiple_of(index[i] * unit, unit), piece.shape[0])
            product = lax.dot_general(
                piece[...], weight[rows, :], (((0,), (0,)), ((), ())), preferred_element_type=f32
            )
            total = product if total is None else total + product
        to[...] = total.astype(to.dtype)


def after(x, event):
    return lax.optimization_barrier((x, event))[0]


def pool_group_out(pool_input, earlier_rows, pool_map, pool_scale, tp_rank, ep_rank):
    row_count, channels = pool_input.shape
    group_dim = pool_map.shape[1]
    local_groups = channels // group_dim
    values = pool_input.astype(f32)
    extended = jnp.concatenate([earlier_rows.astype(f32), values], axis=0)
    position = (ep_rank * row_count + jnp.arange(row_count, dtype=jnp.int32)).astype(f32)
    group_ids = tp_rank * local_groups + jnp.arange(channels, dtype=jnp.int32) // group_dim
    group_kind = group_ids % 4
    running = jnp.zeros((row_count, channels), f32)
    pooled = -values
    for lag_step in range(reach_back + 1):
        running = running + extended[reach_back - lag_step : reach_back - lag_step + row_count]
        if lag_step + 1 in windows:
            kind_id = windows.index(lag_step + 1)
            counts = jnp.minimum(position + 1.0, float(lag_step + 1))
            select = (group_kind == kind_id).astype(f32)
            pooled = pooled + select[None, :] * running / counts[:, None]
    pooled = pooled.astype(bf16)
    my_maps = lax.dynamic_slice_in_dim(pool_map, tp_rank * local_groups, local_groups, 0)
    my_scale = lax.dynamic_slice_in_dim(pool_scale, tp_rank * channels, channels, 0)
    mapped = jnp.einsum(
        "rgc,gcd->rgd",
        pooled.reshape(row_count, local_groups, group_dim),
        my_maps,
        preferred_element_type=f32,
    )
    return (mapped.reshape(row_count, channels) * my_scale[None, :]).astype(bf16)


def per_device(
    pool_input,
    pool_map,
    pool_scale,
    out_proj,
    moe_input,
    norm_gain,
    routes,
    route_weights,
    expert_gate,
    expert_up,
    expert_down,
    shared_gate,
    shared_up,
    shared_down,
):
    tp_rank = lax.axis_index("tp")
    ep_rank = lax.axis_index("ep")
    tp_size = lax.axis_size("tp")
    expert_count = lax.axis_size("ep")
    y_size = tp_size // 2
    core = tp_rank % 2
    y = tp_rank // 2
    tok_count, width = moe_input.shape
    top_count = routes.shape[1]
    capacity = (3 * tok_count * top_count + 2 * expert_count - 1) // (2 * expert_count)
    buffer_len = expert_count * capacity
    slice_width = width // tp_size
    row_count = pool_input.shape[0]

    earlier_rows = halo(pool_input[row_count - reach_back :])

    routes_t = routes.T
    experts = jnp.arange(expert_count, dtype=jnp.int32)[:, None]
    named = jnp.zeros((expert_count, tok_count), f32)
    weight_t = jnp.zeros((expert_count, tok_count), f32)
    for k in range(top_count):
        hit = routes_t[k][None, :] == experts
        named = named + hit.astype(f32)
        weight_t = weight_t + jnp.where(hit, route_weights.T[k][None, :], 0.0)
    before = jnp.arange(tok_count)[:, None] < jnp.arange(tok_count)[None, :]
    earlier = jnp.dot(named.astype(bf16), before.astype(bf16), preferred_element_type=f32)
    slot = jnp.where(named > 0, earlier, -1.0)
    slots = jnp.arange(capacity, dtype=f32)[None, :, None]
    match = slot[:, None, :] == slots
    placing = match.astype(bf16).reshape(buffer_len, tok_count)
    combine = jnp.where(match, weight_t[:, None, :], 0.0).astype(bf16).reshape(buffer_len, tok_count)

    values = moe_input.astype(f32)
    mean = jnp.mean(values, axis=1, keepdims=True)
    centre = values - mean
    rstd = lax.rsqrt(jnp.mean(centre * centre, axis=1, keepdims=True) + eps)

    home = y + core * (y_size // 2)
    chip_width = 2 * slice_width
    at = (home % y_size) * chip_width
    mine = lax.dynamic_slice_in_dim(moe_input, at, chip_width, 1).astype(f32)
    gain = lax.dynamic_slice_in_dim(norm_gain, at, chip_width, 0)
    normed_slice = ((mine - mean) * rstd * gain[None, :]).astype(bf16)

    def exchanged(rows):
        return lax.all_to_all(rows, "ep", split_axis=0, concat_axis=0, tiled=True)

    outgoing = jnp.dot(placing, normed_slice, preferred_element_type=f32).astype(bf16)
    arrived = exchanged(outgoing)
    pool_input = after(pool_input, outgoing)
    upward = jnp.array([4, 3, 2, 1], jnp.int32)
    downward = jnp.array([5, 6, 7, 0], jnp.int32)
    kept_ids = jnp.where(core == 0, downward, upward)
    sent_ids = jnp.where(core == 0, upward, downward)
    index = (y + jnp.stack([kept_ids, sent_ids])) % y_size
    offsets = jnp.where(core == 0, jnp.array([0, -1, 1, -2, 2], jnp.int32), jnp.array([0, 1, -1, 0, 0], jnp.int32))
    near_index = (home + y_size + offsets) % y_size
    near_index = jnp.concatenate([near_index, core[None]]).astype(jnp.int32)

    group_out = pool_group_out(pool_input, earlier_rows, pool_map, pool_scale, tp_rank, ep_rank)
    normed = (centre * rstd * norm_gain[None, :]).astype(bf16)
    shared_gate_val = jnp.dot(normed, shared_gate, preferred_element_type=f32)
    shared_up_val = jnp.dot(normed, shared_up, preferred_element_type=f32)
    shared_hidden = (jax.nn.silu(shared_gate_val) * shared_up_val).astype(bf16)

    shape = jax.ShapeDtypeStruct((y_size // 2, row_count + tok_count, chip_width), bf16)
    kept, given = local_kernel(project_kernel, index, (group_out, shared_hidden, out_proj, shared_down), [shape, shape])
    from_partner = to_partner(given)

    gate_t = expert_gate[0].T
    up_t = expert_up[0].T
    units = gate_t.shape[0]
    blocks = jax.ShapeDtypeStruct((5, 4 * units, chip_width), bf16)
    partner_gate = to_partner(gate_t)
    partner_up = to_partner(up_t)
    own_down = expert_down[0]
    partner_down = to_partner(own_down)
    weights = local_kernel(weight_kernel, near_index, (gate_t, up_t, partner_gate, partner_up), blocks)

    def part(j):
        return kept[j].astype(f32) + from_partner[j].astype(f32)

    def ring_sum(j, ring):
        return (part(j) + ring.astype(f32)).astype(bf16)

    def ring_step(x):
        return sent(x.astype(bf16), {0: (-1, 0), 1: (1, 1)})

    one = sent(arrived, {0: (1, 0), 1: (-1, 1)})
    other = sent(arrived, {0: (-1, 0), 1: (1, 1)})
    up_two = sent(one, {0: (1, 0)})
    down_two = sent(other, {0: (-1, 0)})
    ring = ring_step(part(0))
    ring = ring_step(ring_sum(1, ring))
    summed = tdot(weights[0], arrived)
    for j, rows in enumerate((one, other, up_two, down_two)):
        summed = summed + tdot(weights[j + 1], rows)
    full = summed + to_partner(summed)
    chip_units = 2 * units
    hidden = (jax.nn.silu(full[:chip_units]) * full[chip_units:]).astype(bf16)

    half = jnp.where(core == 0, hidden[:units], hidden[units:])
    side = jnp.where(core == 0, -1, 1)
    pieces = [half]
    begins = [2 * y + core]
    for distance in range(1, y_size // 2 + 1):
        farthest = 2 * distance == y_size
        route = {0: (distance, 0), 1: (-distance, 1)}
        pieces.append(sent(half if farthest else hidden, route))
        begins.append(2 * ((y + y_size + side * distance) % y_size) + (core if farthest else 0))
    sums = [jax.ShapeDtypeStruct((buffer_len, slice_width), kind) for kind in (f32, bf16)]
    own_sum, partner_sum = local_kernel(
        down_kernel, jnp.stack(begins).astype(jnp.int32), (*pieces, own_down, partner_down), sums
    )
    ring = ring_step(ring_sum(2, ring))
    expert_result = own_sum + to_partner(partner_sum).astype(f32)
    expert_result = expert_result.astype(bf16)
    returned = exchanged(expert_result)
    routed = lax.dot_general(combine, returned, (((0,), (0,)), ((), ())), preferred_element_type=f32)

    done = part(3) + ring.astype(f32)
    low = done[:, :slice_width]
    high = done[:, slice_width:]
    cross = sent(jnp.where(core == 0, high, low).astype(bf16), {0: (0, 1), 1: (1, 0)})
    straight = sent(high.astype(bf16), {1: (1, 1)})
    total = cross.astype(f32) + straight.astype(f32) + jnp.where(core == 0, low, 0.0)
    return (total[:row_count].astype(bf16), (routed + total[row_count:]).astype(bf16))


def solution(mesh):
    return jax.shard_map(
        per_device,
        mesh=mesh,
        in_specs=(
            P("ep", "tp"),
            P(),
            P(),
            P("tp", None),
            P("ep", None),
            P(),
            P("ep", None),
            P("ep", None),
            P("ep", None, "tp"),
            P("ep", None, "tp"),
            P("ep", None, "tp"),
            P(None, "tp"),
            P(None, "tp"),
            P("tp", None),
        ),
        out_specs=(P("ep", "tp"), P("ep", "tp")),
        check_vma=False,
    )
```

```python
import jax
import jax.numpy as jnp
from jax import lax
from jax.experimental import pallas as pl
from jax.experimental.pallas import tpu as pltpu
from jax.sharding import PartitionSpec as P


windows = (2, 4, 8, 16)
reach_back = 15
eps = 1e-05
f32 = jnp.float32
bf16 = jnp.bfloat16


def halo(block):
    devices = range(lax.axis_size("ep"))
    return lax.ppermute(block, "ep", [(i - 1, i) for i in devices if i > 0])


def sent(x, targets):
    n = lax.axis_size("tp") // 2
    route = []
    for core, (step, to) in targets.items():
        route += [(2 * i + core, 2 * ((i + step) % n) + to) for i in range(n)]
    return lax.ppermute(x, "tp", route)


def to_partner(x):
    n = lax.axis_size("tp")
    return lax.ppermute(x, "tp", [(i, i ^ 1) for i in range(n)])


def tdot(a, b):
    return lax.dot_general(a, b, (((1,), (1,)), ((), ())), preferred_element_type=f32)


def lanes(block, width):
    return pl.ds(pl.multiple_of(block * width, width), width)


def local_kernel(body, index, operands, out_shape):
    vmem = pl.BlockSpec(memory_space=pltpu.VMEM)
    smem = pl.BlockSpec(memory_space=pltpu.SMEM)
    several = isinstance(out_shape, list)
    return pl.pallas_call(
        body,
        in_specs=[smem] + [vmem] * len(operands),
        out_specs=[vmem] * len(out_shape) if several else vmem,
        out_shape=out_shape,
    )(index, *operands)


def weight_kernel(index, gate, up, partner_gate, partner_up, blocks):
    count, _, width = blocks.shape
    units = gate.shape[0]
    first = index[count] == 0
    for j in range(count):
        at = lanes(index[j], width)
        for i, (own, partner) in enumerate(((gate, partner_gate), (up, partner_up))):
            mine = own[:, at]
            other = partner[:, at]
            low = 2 * i * units
            blocks[j, low : low + units] = jnp.where(first, mine, other)
            blocks[j, low + units : low + 2 * units] = jnp.where(first, other, mine)


def project_kernel(index, group, hidden, proj, down, own, out):
    rows = group.shape[0]
    count, _, width = own.shape
    for side, to in ((1, out), (0, own)):
        for j in range(count):
            at = lanes(index[side, j], width)
            to[j, :rows] = jnp.dot(group[...], proj[:, at], preferred_element_type=f32).astype(bf16)
            to[j, rows:] = jnp.dot(hidden[...], down[:, at], preferred_element_type=f32).astype(bf16)


def down_rows_kernel(index, own, partner, blocks):
    unit = blocks.shape[0] // 8
    width = own.shape[1]
    counts = (1, 2, 2, 2, 1)
    to = 0
    for i, count in enumerate(counts):
        rows = pl.ds(pl.multiple_of(index[i] * unit, unit), count * unit)
        for side, source in enumerate((own, partner)):
            blocks[to : to + count * unit, side * width : (side + 1) * width] = source[rows, :]
        to += count * unit


def down_kernel(*refs):
    *pieces, blocks, own_sum, partner_sum, joined = refs
    to = 0
    for piece in pieces:
        count = piece.shape[0]
        joined[to : to + count, :] = piece[...]
        to += count
    width = own_sum.shape[1]
    for part, out in enumerate((own_sum, partner_sum)):
        weight = blocks[:, part * width : (part + 1) * width]
        product = lax.dot_general(joined[...], weight, (((0,), (0,)), ((), ())), preferred_element_type=f32)
        out[...] = product.astype(out.dtype)


def after(x, event):
    return lax.optimization_barrier((x, event))[0]


def pool_group_out(pool_input, earlier_rows, pool_map, pool_scale, tp_rank, ep_rank):
    row_count, channels = pool_input.shape
    group_dim = pool_map.shape[1]
    local_groups = channels // group_dim
    values = pool_input.astype(f32)
    extended = jnp.concatenate([earlier_rows.astype(f32), values], axis=0)
    position = (ep_rank * row_count + jnp.arange(row_count, dtype=jnp.int32)).astype(f32)
    group_ids = tp_rank * local_groups + jnp.arange(channels, dtype=jnp.int32) // group_dim
    group_kind = group_ids % 4
    running = jnp.zeros((row_count, channels), f32)
    pooled = -values
    for lag_step in range(reach_back + 1):
        running = running + extended[reach_back - lag_step : reach_back - lag_step + row_count]
        if lag_step + 1 in windows:
            kind_id = windows.index(lag_step + 1)
            counts = jnp.minimum(position + 1.0, float(lag_step + 1))
            select = (group_kind == kind_id).astype(f32)
            pooled = pooled + select[None, :] * running / counts[:, None]
    pooled = pooled.astype(bf16)
    my_maps = lax.dynamic_slice_in_dim(pool_map, tp_rank * local_groups, local_groups, 0)
    my_scale = lax.dynamic_slice_in_dim(pool_scale, tp_rank * channels, channels, 0)
    mapped = jnp.einsum(
        "rgc,gcd->rgd",
        pooled.reshape(row_count, local_groups, group_dim),
        my_maps,
        preferred_element_type=f32,
    )
    return (mapped.reshape(row_count, channels) * my_scale[None, :]).astype(bf16)


def per_device(
    pool_input,
    pool_map,
    pool_scale,
    out_proj,
    moe_input,
    norm_gain,
    routes,
    route_weights,
    expert_gate,
    expert_up,
    expert_down,
    shared_gate,
    shared_up,
    shared_down,
):
    tp_rank = lax.axis_index("tp")
    ep_rank = lax.axis_index("ep")
    tp_size = lax.axis_size("tp")
    expert_count = lax.axis_size("ep")
    y_size = tp_size // 2
    core = tp_rank % 2
    y = tp_rank // 2
    tok_count, width = moe_input.shape
    top_count = routes.shape[1]
    capacity = (3 * tok_count * top_count + 2 * expert_count - 1) // (2 * expert_count)
    buffer_len = expert_count * capacity
    slice_width = width // tp_size
    row_count = pool_input.shape[0]

    earlier_rows = halo(pool_input[row_count - reach_back :])

    values = moe_input.astype(f32)
    mean = jnp.mean(values, axis=1, keepdims=True)
    routes = after(routes, mean)
    centre = values - mean
    rstd = lax.rsqrt(jnp.mean(centre * centre, axis=1, keepdims=True) + eps)

    routes_t = routes.T
    experts = jnp.arange(expert_count, dtype=jnp.int32)[:, None]
    named = jnp.zeros((expert_count, tok_count), f32)
    weight_t = jnp.zeros((expert_count, tok_count), f32)
    for k in range(top_count):
        hit = routes_t[k][None, :] == experts
        named = named + hit.astype(f32)
        weight_t = weight_t + jnp.where(hit, route_weights.T[k][None, :], 0.0)
    before = jnp.arange(tok_count)[:, None] < jnp.arange(tok_count)[None, :]
    earlier = jnp.dot(named.astype(bf16), before.astype(bf16), preferred_element_type=f32)
    slot = jnp.where(named > 0, earlier, -1.0)
    slots = jnp.arange(capacity, dtype=f32)[None, :, None]
    match = slot[:, None, :] == slots
    placing = match.astype(bf16).reshape(buffer_len, tok_count)
    combine = jnp.where(match, weight_t[:, None, :], 0.0).astype(bf16).reshape(buffer_len, tok_count)


    home = y + core * (y_size // 2)
    chip_width = 2 * slice_width
    at = (home % y_size) * chip_width
    mine = lax.dynamic_slice_in_dim(moe_input, at, chip_width, 1).astype(f32)
    gain = lax.dynamic_slice_in_dim(norm_gain, at, chip_width, 0)
    normed_slice = ((mine - mean) * rstd * gain[None, :]).astype(bf16)

    def exchanged(rows):
        return lax.all_to_all(rows, "ep", split_axis=0, concat_axis=0, tiled=True)

    outgoing = jnp.dot(placing, normed_slice, preferred_element_type=f32).astype(bf16)
    arrived = exchanged(outgoing)
    pool_input = after(pool_input, outgoing)
    upward = jnp.array([4, 3, 2, 1], jnp.int32)
    downward = jnp.array([5, 6, 7, 0], jnp.int32)
    kept_ids = jnp.where(core == 0, downward, upward)
    sent_ids = jnp.where(core == 0, upward, downward)
    index = (y + jnp.stack([kept_ids, sent_ids])) % y_size
    offsets = jnp.where(core == 0, jnp.array([0, -1, 1, -2, 2], jnp.int32), jnp.array([0, 1, -1, 0, 0], jnp.int32))
    near_index = (home + y_size + offsets) % y_size
    near_index = jnp.concatenate([near_index, core[None]]).astype(jnp.int32)

    group_out = pool_group_out(pool_input, earlier_rows, pool_map, pool_scale, tp_rank, ep_rank)
    normed = (centre * rstd * norm_gain[None, :]).astype(bf16)
    shared_gate_val = jnp.dot(normed, shared_gate, preferred_element_type=f32)
    shared_up_val = jnp.dot(normed, shared_up, preferred_element_type=f32)
    shared_hidden = (jax.nn.silu(shared_gate_val) * shared_up_val).astype(bf16)

    shape = pltpu.VMEM((y_size // 2, row_count + tok_count, chip_width), bf16)
    kept, given = local_kernel(project_kernel, index, (group_out, shared_hidden, out_proj, shared_down), [shape, shape])
    from_partner = to_partner(given)

    gate_t = expert_gate[0].T
    up_t = expert_up[0].T
    units = gate_t.shape[0]
    blocks = pltpu.VMEM((5, 4 * units, chip_width), bf16)
    partner_gate = to_partner(gate_t)
    partner_up = to_partner(up_t)
    own_down = expert_down[0]
    partner_down = to_partner(own_down)
    weights = local_kernel(weight_kernel, near_index, (gate_t, up_t, partner_gate, partner_up), blocks)

    def part(j):
        return kept[j].astype(f32) + from_partner[j].astype(f32)

    def ring_sum(j, ring):
        return (part(j) + ring.astype(f32)).astype(bf16)

    def ring_step(x):
        return sent(x.astype(bf16), {0: (-1, 0), 1: (1, 1)})

    one = sent(arrived, {0: (1, 0), 1: (-1, 1)})
    other = sent(arrived, {0: (-1, 0), 1: (1, 1)})
    up_two = sent(one, {0: (1, 0)})
    down_two = sent(other, {0: (-1, 0)})
    ring = ring_step(part(0))
    ring = ring_step(ring_sum(1, ring))
    summed = tdot(weights[0], arrived)
    for j, rows in enumerate((one, other, up_two, down_two)):
        summed = summed + tdot(weights[j + 1], rows)
    full = summed + to_partner(summed)
    chip_units = 2 * units
    hidden = (jax.nn.silu(full[:chip_units]) * full[chip_units:]).astype(bf16)

    half = jnp.where(core == 0, hidden[:units], hidden[units:])
    side = jnp.where(core == 0, -1, 1)
    pieces = [half]
    begins = [2 * y + core]
    for distance in range(1, y_size // 2 + 1):
        farthest = 2 * distance == y_size
        route = {0: (distance, 0), 1: (-distance, 1)}
        pieces.append(sent(half if farthest else hidden, route))
        begins.append(2 * ((y + y_size + side * distance) % y_size) + (core if farthest else 0))
    blocks = pltpu.VMEM((y_size * units, 2 * slice_width), bf16)
    rows_index = jnp.stack(begins).astype(jnp.int32)
    down_blocks = local_kernel(down_rows_kernel, rows_index, (own_down, partner_down), blocks)
    vmem = pl.BlockSpec(memory_space=pltpu.VMEM)
    own_sum, partner_sum = pl.pallas_call(
        down_kernel,
        in_specs=[vmem] * (len(pieces) + 1),
        out_specs=[vmem] * 2,
        out_shape=[pltpu.VMEM((buffer_len, slice_width), kind) for kind in (f32, bf16)],
        scratch_shapes=[pltpu.VMEM((y_size * units, buffer_len), bf16)],
    )(*[pltpu.with_memory_space_constraint(a, pltpu.VMEM) for a in (*pieces, down_blocks)])
    ring = ring_step(ring_sum(2, ring))
    expert_result = own_sum + to_partner(partner_sum).astype(f32)
    expert_result = expert_result.astype(bf16)
    returned = exchanged(expert_result)
    routed = lax.dot_general(combine, returned, (((0,), (0,)), ((), ())), preferred_element_type=f32)

    done = part(3) + ring.astype(f32)
    low = done[:, :slice_width]
    high = done[:, slice_width:]
    cross = sent(jnp.where(core == 0, high, low).astype(bf16), {0: (0, 1), 1: (1, 0)})
    straight = sent(high.astype(bf16), {1: (1, 1)})
    total = cross.astype(f32) + straight.astype(f32) + jnp.where(core == 0, low, 0.0)
    return (total[:row_count].astype(bf16), (routed + total[row_count:]).astype(bf16))


def solution(mesh):
    return jax.shard_map(
        per_device,
        mesh=mesh,
        in_specs=(
            P("ep", "tp"),
            P(),
            P(),
            P("tp", None),
            P("ep", None),
            P(),
            P("ep", None),
            P("ep", None),
            P("ep", None, "tp"),
            P("ep", None, "tp"),
            P("ep", None, "tp"),
            P(None, "tp"),
            P(None, "tp"),
            P("tp", None),
        ),
        out_specs=(P("ep", "tp"), P("ep", "tp")),
        check_vma=False,
    )
```

```python
import jax
import jax.numpy as jnp
from jax import lax
from jax.experimental import pallas as pl
from jax.experimental.pallas import tpu as pltpu
from jax.sharding import PartitionSpec as P


windows = (2, 4, 8, 16)
reach_back = 15
eps = 1e-05
f32 = jnp.float32
bf16 = jnp.bfloat16
grant = pltpu.CompilerParams(vmem_limit_bytes=16 * 1024 * 1024)


def halo(block):
    devices = range(lax.axis_size("ep"))
    return lax.ppermute(block, "ep", [(i - 1, i) for i in devices if i > 0])


def sent(x, targets):
    n = lax.axis_size("tp") // 2
    route = []
    for core, (step, to) in targets.items():
        route += [(2 * i + core, 2 * ((i + step) % n) + to) for i in range(n)]
    return lax.ppermute(x, "tp", route)


def to_partner(x):
    n = lax.axis_size("tp")
    return lax.ppermute(x, "tp", [(i, i ^ 1) for i in range(n)])


def tdot(a, b):
    return lax.dot_general(a, b, (((1,), (1,)), ((), ())), preferred_element_type=f32)


def lanes(block, width):
    return pl.ds(pl.multiple_of(block * width, width), width)


def local_kernel(body, index, operands, out_shape):
    vmem = pl.BlockSpec(memory_space=pltpu.VMEM)
    smem = pl.BlockSpec(memory_space=pltpu.SMEM)
    several = isinstance(out_shape, list)
    return pl.pallas_call(
        body,
        in_specs=[smem] + [vmem] * len(operands),
        out_specs=[vmem] * len(out_shape) if several else vmem,
        out_shape=out_shape,
        compiler_params=grant,
    )(index, *operands)


def weight_kernel(index, gate, up, partner_gate, partner_up, blocks):
    count, _, width = blocks.shape
    units = gate.shape[0]
    first = index[count] == 0
    for j in range(count):
        at = lanes(index[j], width)
        for i, (own, partner) in enumerate(((gate, partner_gate), (up, partner_up))):
            mine = own[:, at]
            other = partner[:, at]
            low = 2 * i * units
            blocks[j, low : low + units] = jnp.where(first, mine, other)
            blocks[j, low + units : low + 2 * units] = jnp.where(first, other, mine)


def project_kernel(index, group, hidden, proj, down, own, out):
    rows = group.shape[0]
    count, _, width = own.shape
    for side, to in ((1, out), (0, own)):
        for j in range(count):
            at = lanes(index[side, j], width)
            to[j, :rows] = jnp.dot(group[...], proj[:, at], preferred_element_type=f32).astype(bf16)
            to[j, rows:] = jnp.dot(hidden[...], down[:, at], preferred_element_type=f32).astype(bf16)


def in_vmem(body, operands, out_shape, **options):
    vmem = pl.BlockSpec(memory_space=pltpu.VMEM)
    several = isinstance(out_shape, list)
    return pl.pallas_call(
        body,
        in_specs=[vmem] * len(operands),
        out_specs=[vmem] * len(out_shape) if several else vmem,
        out_shape=out_shape,
        compiler_params=grant,
        **options,
    )(*[pltpu.with_memory_space_constraint(a, pltpu.VMEM) for a in operands])


def rows_sum(weights, chunks, first, base):
    rows = chunks[0].shape[0]
    step = rows // 3

    def body(*refs):
        weight, *sources, out = refs
        before = sources.pop() if base is not None else None
        for lo in range(0, rows, step):
            total = None if before is None else before[:, lo : lo + step]
            for i, source in enumerate(sources):
                product = tdot(weight[first + i], source[lo : lo + step, :])
                total = product if total is None else total + product
            out[:, lo : lo + step] = total

    operands = [weights, *chunks] + ([] if base is None else [base])
    return in_vmem(body, operands, pltpu.VMEM((weights.shape[1], rows), f32))


def gate_kernel(mine, other, hidden):
    units = hidden.shape[0]
    gate = mine[:units] + other[:units]
    up = mine[units:] + other[units:]
    hidden[...] = (jax.nn.silu(gate) * up).astype(bf16)


def down_rows_kernel(index, own, partner, blocks):
    unit = blocks.shape[0] // 8
    width = own.shape[1]
    counts = (1, 2, 2, 2, 1)
    to = 0
    for i, count in enumerate(counts):
        rows = pl.ds(pl.multiple_of(index[i] * unit, unit), count * unit)
        for side, source in enumerate((own, partner)):
            blocks[to : to + count * unit, side * width : (side + 1) * width] = source[rows, :]
        to += count * unit


def down_kernel(*refs):
    *pieces, blocks, own_sum, partner_sum, joined = refs
    to = 0
    for piece in pieces:
        count = piece.shape[0]
        joined[to : to + count, :] = piece[...]
        to += count
    width = own_sum.shape[1]
    for part, out in enumerate((own_sum, partner_sum)):
        weight = blocks[:, part * width : (part + 1) * width]
        product = lax.dot_general(joined[...], weight, (((0,), (0,)), ((), ())), preferred_element_type=f32)
        out[...] = product.astype(out.dtype)


def after(x, event):
    return lax.optimization_barrier((x, event))[0]


def pool_group_out(pool_input, earlier_rows, pool_map, pool_scale, tp_rank, ep_rank):
    row_count, channels = pool_input.shape
    group_dim = pool_map.shape[1]
    local_groups = channels // group_dim
    values = pool_input.astype(f32)
    extended = jnp.concatenate([earlier_rows.astype(f32), values], axis=0)
    position = (ep_rank * row_count + jnp.arange(row_count, dtype=jnp.int32)).astype(f32)
    group_ids = tp_rank * local_groups + jnp.arange(channels, dtype=jnp.int32) // group_dim
    group_kind = group_ids % 4
    running = jnp.zeros((row_count, channels), f32)
    pooled = -values
    for lag_step in range(reach_back + 1):
        running = running + extended[reach_back - lag_step : reach_back - lag_step + row_count]
        if lag_step + 1 in windows:
            kind_id = windows.index(lag_step + 1)
            counts = jnp.minimum(position + 1.0, float(lag_step + 1))
            select = (group_kind == kind_id).astype(f32)
            pooled = pooled + select[None, :] * running / counts[:, None]
    pooled = pooled.astype(bf16)
    my_maps = lax.dynamic_slice_in_dim(pool_map, tp_rank * local_groups, local_groups, 0)
    my_scale = lax.dynamic_slice_in_dim(pool_scale, tp_rank * channels, channels, 0)
    mapped = jnp.einsum(
        "rgc,gcd->rgd",
        pooled.reshape(row_count, local_groups, group_dim),
        my_maps,
        preferred_element_type=f32,
    )
    return (mapped.reshape(row_count, channels) * my_scale[None, :]).astype(bf16)


def per_device(
    pool_input,
    pool_map,
    pool_scale,
    out_proj,
    moe_input,
    norm_gain,
    routes,
    route_weights,
    expert_gate,
    expert_up,
    expert_down,
    shared_gate,
    shared_up,
    shared_down,
):
    tp_rank = lax.axis_index("tp")
    ep_rank = lax.axis_index("ep")
    tp_size = lax.axis_size("tp")
    expert_count = lax.axis_size("ep")
    y_size = tp_size // 2
    core = tp_rank % 2
    y = tp_rank // 2
    tok_count, width = moe_input.shape
    top_count = routes.shape[1]
    capacity = (3 * tok_count * top_count + 2 * expert_count - 1) // (2 * expert_count)
    buffer_len = expert_count * capacity
    slice_width = width // tp_size
    row_count = pool_input.shape[0]

    earlier_rows = halo(pool_input[row_count - reach_back :])

    values = moe_input.astype(f32)
    mean = jnp.mean(values, axis=1, keepdims=True)
    routes = after(routes, mean)
    centre = values - mean
    rstd = lax.rsqrt(jnp.mean(centre * centre, axis=1, keepdims=True) + eps)

    routes_t = routes.T
    experts = jnp.arange(expert_count, dtype=jnp.int32)[:, None]
    named = jnp.zeros((expert_count, tok_count), f32)
    weight_t = jnp.zeros((expert_count, tok_count), f32)
    for k in range(top_count):
        hit = routes_t[k][None, :] == experts
        named = named + hit.astype(f32)
        weight_t = weight_t + jnp.where(hit, route_weights.T[k][None, :], 0.0)
    before = jnp.arange(tok_count)[:, None] < jnp.arange(tok_count)[None, :]
    earlier = jnp.dot(named.astype(bf16), before.astype(bf16), preferred_element_type=f32)
    slot = jnp.where(named > 0, earlier, -1.0)
    slots = jnp.arange(capacity, dtype=f32)[None, :, None]
    match = slot[:, None, :] == slots
    placing = match.astype(bf16).reshape(buffer_len, tok_count)
    combine = jnp.where(match, weight_t[:, None, :], 0.0).astype(bf16).reshape(buffer_len, tok_count)


    home = y + core * (y_size // 2)
    chip_width = 2 * slice_width
    at = (home % y_size) * chip_width
    mine = lax.dynamic_slice_in_dim(moe_input, at, chip_width, 1).astype(f32)
    gain = lax.dynamic_slice_in_dim(norm_gain, at, chip_width, 0)
    normed_slice = ((mine - mean) * rstd * gain[None, :]).astype(bf16)

    def exchanged(rows):
        return lax.all_to_all(rows, "ep", split_axis=0, concat_axis=0, tiled=True)

    outgoing = jnp.dot(placing, normed_slice, preferred_element_type=f32).astype(bf16)
    arrived = exchanged(outgoing)
    pool_input = after(pool_input, outgoing)
    upward = jnp.array([4, 3, 2, 1], jnp.int32)
    downward = jnp.array([5, 6, 7, 0], jnp.int32)
    kept_ids = jnp.where(core == 0, downward, upward)
    sent_ids = jnp.where(core == 0, upward, downward)
    index = (y + jnp.stack([kept_ids, sent_ids])) % y_size
    offsets = jnp.where(core == 0, jnp.array([0, -1, 1, -2, 2], jnp.int32), jnp.array([0, 1, -1, 0, 0], jnp.int32))
    near_index = (home + y_size + offsets) % y_size
    near_index = jnp.concatenate([near_index, core[None]]).astype(jnp.int32)

    group_out = pool_group_out(pool_input, earlier_rows, pool_map, pool_scale, tp_rank, ep_rank)
    normed = (centre * rstd * norm_gain[None, :]).astype(bf16)
    shared_gate_val = jnp.dot(normed, shared_gate, preferred_element_type=f32)
    shared_up_val = jnp.dot(normed, shared_up, preferred_element_type=f32)
    shared_hidden = (jax.nn.silu(shared_gate_val) * shared_up_val).astype(bf16)

    shape = pltpu.VMEM((y_size // 2, row_count + tok_count, chip_width), bf16)
    kept, given = local_kernel(project_kernel, index, (group_out, shared_hidden, out_proj, shared_down), [shape, shape])
    from_partner = to_partner(given)

    gate_t = expert_gate[0].T
    up_t = expert_up[0].T
    units = gate_t.shape[0]
    blocks = pltpu.VMEM((5, 4 * units, chip_width), bf16)
    partner_gate = to_partner(gate_t)
    partner_up = to_partner(up_t)
    own_down = expert_down[0]
    partner_down = to_partner(own_down)
    weights = local_kernel(weight_kernel, near_index, (gate_t, up_t, partner_gate, partner_up), blocks)

    def part(j):
        return kept[j].astype(f32) + from_partner[j].astype(f32)

    def ring_sum(j, ring):
        return (part(j) + ring.astype(f32)).astype(bf16)

    def ring_step(x):
        return sent(x.astype(bf16), {0: (-1, 0), 1: (1, 1)})

    one = sent(arrived, {0: (1, 0), 1: (-1, 1)})
    other = sent(arrived, {0: (-1, 0), 1: (1, 1)})
    up_two = sent(one, {0: (1, 0)})
    down_two = sent(other, {0: (-1, 0)})
    ring = ring_step(part(0))
    ring = ring_step(ring_sum(1, ring))
    summed = rows_sum(weights, (arrived,), 0, None)
    summed = rows_sum(weights, (one, other), 1, summed)
    summed = rows_sum(weights, (up_two, down_two), 3, summed)
    chip_units = 2 * units
    shape = pltpu.VMEM((chip_units, buffer_len), bf16)
    hidden = in_vmem(gate_kernel, (summed, to_partner(summed)), shape)

    half = jnp.where(core == 0, hidden[:units], hidden[units:])
    side = jnp.where(core == 0, -1, 1)
    pieces = [half]
    begins = [2 * y + core]
    for distance in range(1, y_size // 2 + 1):
        farthest = 2 * distance == y_size
        route = {0: (distance, 0), 1: (-distance, 1)}
        pieces.append(sent(half if farthest else hidden, route))
        begins.append(2 * ((y + y_size + side * distance) % y_size) + (core if farthest else 0))
    blocks = pltpu.VMEM((y_size * units, 2 * slice_width), bf16)
    rows_index = jnp.stack(begins).astype(jnp.int32)
    down_blocks = local_kernel(down_rows_kernel, rows_index, (own_down, partner_down), blocks)
    own_sum, partner_sum = in_vmem(
        down_kernel,
        (*pieces, down_blocks),
        [pltpu.VMEM((buffer_len, slice_width), kind) for kind in (f32, bf16)],
        scratch_shapes=[pltpu.VMEM((y_size * units, buffer_len), bf16)],
    )
    ring = ring_step(ring_sum(2, ring))
    expert_result = own_sum + to_partner(partner_sum).astype(f32)
    expert_result = expert_result.astype(bf16)
    returned = exchanged(expert_result)
    routed = lax.dot_general(combine, returned, (((0,), (0,)), ((), ())), preferred_element_type=f32)

    done = part(3) + ring.astype(f32)
    low = done[:, :slice_width]
    high = done[:, slice_width:]
    cross = sent(jnp.where(core == 0, high, low).astype(bf16), {0: (0, 1), 1: (1, 0)})
    straight = sent(high.astype(bf16), {1: (1, 1)})
    total = cross.astype(f32) + straight.astype(f32) + jnp.where(core == 0, low, 0.0)
    return (total[:row_count].astype(bf16), (routed + total[row_count:]).astype(bf16))


def solution(mesh):
    return jax.shard_map(
        per_device,
        mesh=mesh,
        in_specs=(
            P("ep", "tp"),
            P(),
            P(),
            P("tp", None),
            P("ep", None),
            P(),
            P("ep", None),
            P("ep", None),
            P("ep", None, "tp"),
            P("ep", None, "tp"),
            P("ep", None, "tp"),
            P(None, "tp"),
            P(None, "tp"),
            P("tp", None),
        ),
        out_specs=(P("ep", "tp"), P("ep", "tp")),
        check_vma=False,
    )
```
